512 devices in a mesh: grp: 2 (over y), dp: 8 (over x), kv: 16 (over z), tp: 2 (over core).
Axes of the slice: x: 8, y: 2, z: 16, core: 2. Of those that a mesh axis runs over, the one named last changes fastest.
The devices are a block of a 8x8x16 slice.
Arguments:
- tokens: bfloat16 [1024, 4, 4096], P(('grp', 'dp'), None, ('kv', 'tp')), parts along dimension 0, may hold values from -160 to 160
- norm_gain: float32 [4096], replicated, may hold values from 0.1 to 1.9
- w_query: bfloat16 [4096, 16, 64], P(None, 'kv'), may hold values from -0.09375 to 0.09375
- w_key: bfloat16 [4096, 16, 64], P(None, 'kv'), may hold values from -0.09375 to 0.09375
- w_value: bfloat16 [4096, 16, 128], P(None, 'kv', 'tp'), may hold values from -0.09375 to 0.09375
- w_outgate: bfloat16 [4096, 16, 128], P(None, 'kv', 'tp'), may hold values from -0.09375 to 0.09375
- w_input: bfloat16 [4096, 16], replicated, may hold values from -0.09375 to 0.09375
- w_forget: bfloat16 [4096, 16], replicated, may hold values from -0.09375 to 0.09375
- forget_bias: float32 [16], replicated, may hold values from -1 to 4
- head_gain: float32 [16, 128], replicated, may hold values from 0.1 to 1.9
- w_out: bfloat16 [16, 128, 4096], P('kv', 'tp'), may hold values from -0.125 to 0.125
- memory: float32 [1024, 16, 128, 64], P(('grp', 'dp'), 'kv', 'tp'), parts along dimension 0, may hold values from -12 to 12
- normalizer: float32 [1024, 16, 64], P(('grp', 'dp'), 'kv'), parts along dimension 0, may hold values from -12 to 12
- stabilizer: float32 [1024, 16], P(('grp', 'dp'), 'kv'), parts along dimension 0, may hold values from -1 to 1
- prev_keys: bfloat16 [1024, 4, 16, 64], P(('grp', 'dp'), None, 'kv'), parts along dimension 0, may hold values from -6 to 6
- prev_values: bfloat16 [1024, 4, 16, 128], P(('grp', 'dp'), None, 'kv', 'tp'), parts along dimension 0, may hold values from -6 to 6
- prev_input: float32 [1024, 4, 16], P(('grp', 'dp'), None, 'kv'), parts along dimension 0, may hold values from -4 to 4
- prev_forget: float32 [1024, 4, 16], P(('grp', 'dp'), None, 'kv'), parts along dimension 0, may hold values from -2 to -0.02
- accepted: int32 [1024], P(('grp', 'dp')), parts along dimension 0, may hold values from 0 to 4
Outputs:
- mixed: bfloat16 [1024, 4, 4096], P(('grp', 'dp'), None, ('kv', 'tp')), parts along dimension 0
- new_memory: float32 [1024, 16, 128, 64], P(('grp', 'dp'), 'kv', 'tp'), parts along dimension 0
- new_normalizer: float32 [1024, 16, 64], P(('grp', 'dp'), 'kv'), parts along dimension 0
- new_stabilizer: float32 [1024, 16], P(('grp', 'dp'), 'kv'), parts along dimension 0
- new_keys: bfloat16 [1024, 4, 16, 64], P(('grp', 'dp'), None, 'kv'), parts along dimension 0
- new_values: bfloat16 [1024, 4, 16, 128], P(('grp', 'dp'), None, 'kv', 'tp'), parts along dimension 0
- new_input: float32 [1024, 4, 16], P(('grp', 'dp'), None, 'kv'), parts along dimension 0
- new_forget: float32 [1024, 4, 16], P(('grp', 'dp'), None, 'kv'), parts along dimension 0
The draws below stay inside these ranges and needn't reach their ends.
There are 2 independent parts, one for each index of `grp`. The reference program is written for one: setup_inputs(seed, part) draws one part's arguments, and reference() takes and returns one part's arrays. A program takes and returns all parts, laid end to end along the dimension named above; an argument that names none is the same for every part. Nothing has to cross between parts.
All inputs are finite; a program needn't handle non-finite values.
Results may differ from the reference program's by a relative error of at most 0.038.
Values may be sent and summed in bfloat16 or wider, within the bound.
No kernel may reach another device: no remote copies, remote signals or barrier semaphores. Data moves between devices by JAX's collectives and lax.ppermute only.
A program may use at most 64 MiB of HBM per device.

```python
import math
import jax
import jax.numpy as jnp
from jax import lax

D = 4096
HEADS = 16
DK = 64
DV = 128
PROPOSALS = 4
SEQS = 512


def draw_tokens(key, part):
    base_key, row_key = jax.random.split(jax.random.fold_in(key, 17))
    position = jnp.arange(D, dtype=jnp.float32) / (D - 1)
    base = jnp.clip(jax.random.normal(base_key, (SEQS, PROPOSALS, D), jnp.float32), -4.0, 4.0)
    column = jnp.exp(math.log(3.0) * position)
    row_scale = jnp.exp(jax.random.uniform(row_key, (SEQS, PROPOSALS, 1), jnp.float32, 0.0, math.log(10.0)))
    return (base * column * row_scale).astype(jnp.bfloat16)


def with_ends(result, stream_key, low, largest):
    extent = result.shape
    place = [jax.random.randint(jax.random.fold_in(stream_key, axis), (), 0, extent[axis]) for axis in range(len(extent))]
    result = result.at[tuple(place)].set(low)
    longest = extent.index(max(extent))
    place[longest] = (place[longest] + 1) % extent[longest]
    return result.at[tuple(place)].set(largest)


def block_scale(own_key, shape, shards, least, high):
    def one(dim, shards_of):
        heights = jax.random.uniform(jax.random.fold_in(jax.random.fold_in(own_key, 6), dim), (shards_of,), jnp.float32, least / len(shards), high / len(shards))
        return jnp.repeat(jnp.exp(heights), shape[dim] // shards_of).reshape((-1,) + (1,) * (len(shape) - dim - 1))

    gain = one(*shards[0])
    for cut in shards[1:]:
        gain = gain * one(*cut)
    return gain


def bell_draw(key, extent, scale, reach, shards=(), kind=jnp.bfloat16):
    values = jax.random.normal(key, extent, jnp.float32) * scale
    if len(shards) > 0:
        values = block_scale(key, extent, shards, -0.22, 0.18) * values
    return jnp.clip(values, min=-reach, max=reach).astype(kind)


def setup_inputs(seed: int = 0, part: int = 0) -> dict:
    key_list = jax.random.split(jax.random.key(seed), 20)
    own_keys = jax.random.split(jax.random.fold_in(key_list[19], part), 20)
    tokens = draw_tokens(jax.random.fold_in(jax.random.fold_in(key_list[19], part), 71), part)
    norm_gain = jnp.clip(1.0 + 0.18 * jax.random.normal(key_list[1], (D,), jnp.float32), 0.1, 1.9)
    w_query = bell_draw(key_list[2], (D, HEADS, DK), D ** -0.5, 0.09375, ((1, 16),))
    w_key = bell_draw(key_list[3], (D, HEADS, DK), D ** -0.5, 0.09375, ((1, 16),))
    w_value = bell_draw(key_list[4], (D, HEADS, DV), D ** -0.5, 0.09375, ((1, 16), (2, 2)))
    w_outgate = bell_draw(key_list[5], (D, HEADS, DV), D ** -0.5, 0.09375, ((1, 16), (2, 2)))
    w_input = bell_draw(key_list[6], (D, HEADS), D ** -0.5, 0.09375)
    w_forget = bell_draw(key_list[7], (D, HEADS), D ** -0.5, 0.09375)
    forget_bias = jnp.clip(jax.random.uniform(key_list[8], (HEADS,), jnp.float32, -1.0, 4.0), -1.0, 4.0)
    head_gain = jnp.clip(1.0 + 0.18 * jax.random.normal(key_list[9], (HEADS, DV), jnp.float32), 0.1, 1.9)
    w_out = bell_draw(key_list[10], (HEADS, DV, D), (HEADS * DV) ** -0.5, 0.125, ((0, 16), (1, 2)))
    memory = bell_draw(own_keys[11], (SEQS, HEADS, DV, DK), 2.0, 12.0, ((0, 8), (1, 16), (2, 2)), jnp.float32)
    normalizer = bell_draw(own_keys[12], (SEQS, HEADS, DK), 2.0, 12.0, ((0, 8), (1, 16)), jnp.float32)
    stabilizer = jnp.clip(jax.random.uniform(own_keys[13], (SEQS, HEADS), jnp.float32, -1.0, 1.0) * block_scale(own_keys[13], (SEQS, HEADS), ((0, 8), (1, 16)), -0.4, 0.0), -1.0, 1.0)
    prev_keys = bell_draw(own_keys[14], (SEQS, PROPOSALS, HEADS, DK), 1.0, 6.0, ((0, 8), (2, 16)))
    prev_values = bell_draw(own_keys[15], (SEQS, PROPOSALS, HEADS, DV), 1.0, 6.0, ((0, 8), (2, 16), (3, 2)))
    prev_input = bell_draw(own_keys[16], (SEQS, PROPOSALS, HEADS), 1.0, 4.0, ((0, 8), (2, 16)), jnp.float32)
    prev_forget = jnp.clip(-2.0 + 1.98 * jax.random.uniform(own_keys[17], (SEQS, PROPOSALS, HEADS), jnp.float32) ** block_scale(own_keys[17], (SEQS, PROPOSALS, HEADS), ((0, 8), (2, 16)), -0.2, 0.2), -2.0, -0.02)
    accepted = with_ends(jax.random.randint(own_keys[18], (SEQS,), 0, PROPOSALS + 1), jax.random.fold_in(own_keys[18], 1), 0, PROPOSALS).astype(jnp.int32)
    return dict(tokens=tokens, norm_gain=norm_gain, w_query=w_query, w_key=w_key, w_value=w_value, w_outgate=w_outgate, w_input=w_input, w_forget=w_forget, forget_bias=forget_bias, head_gain=head_gain, w_out=w_out, memory=memory, normalizer=normalizer, stabilizer=stabilizer, prev_keys=prev_keys, prev_values=prev_values, prev_input=prev_input, prev_forget=prev_forget, accepted=accepted)


EPS = 1e-06
FAR_NEGATIVE = -1e+30
HIGHEST_PRECISION = lax.Precision.HIGHEST

def recurrent(query_f, key_all, value_all, gate_in, gate_forget, accepted, memory, normalizer, stabilizer):
    proposals = query_f.shape[1]
    total_span = key_all.shape[1]
    position = jnp.arange(total_span, dtype=jnp.int32)
    dropped = (position[None, :] < proposals) & (position[None, :] >= accepted[:, None])
    forget = jnp.where(dropped[:, :, None], 0.0, gate_forget)
    inflow = jnp.where(dropped[:, :, None], FAR_NEGATIVE, gate_in)
    running = jnp.cumsum(forget, axis=1)
    latest = running[:, proposals:]
    spread = latest[:, :, None, :] - running[:, None, :, :] + inflow[:, None, :, :]
    causal = position[None, :] <= (proposals + jnp.arange(proposals, dtype=jnp.int32))[:, None]
    spread = jnp.where(causal[None, :, :, None], spread, FAR_NEGATIVE)
    carried = latest + stabilizer[:, None, :]
    ceiling = jnp.maximum(lax.optimization_barrier(jnp.max(spread, axis=2)), carried)
    scores = jnp.einsum('sthk,suhk->stuh', query_f, key_all, precision=HIGHEST_PRECISION)
    weights = jnp.exp(spread - ceiling[:, :, None, :]) * scores
    carry_scale = jnp.exp(carried - ceiling)
    numerator = jnp.einsum('stuh,suhv->sthv', weights, value_all, precision=HIGHEST_PRECISION)
    numerator = numerator + carry_scale[..., None] * jnp.einsum('shvk,sthk->sthv', memory, query_f, precision=HIGHEST_PRECISION)
    denominator = lax.optimization_barrier(jnp.sum(weights, axis=2)) + carry_scale * jnp.einsum('shk,sthk->sth', normalizer, query_f, precision=HIGHEST_PRECISION)
    cell_out = numerator / jnp.maximum(jnp.abs(denominator), jnp.exp(-ceiling))[..., None]
    boundary = running[:, proposals - 1]
    reached = boundary[:, None, :] - running[:, :proposals] + inflow[:, :proposals]
    new_stabilizer = jnp.maximum(boundary + stabilizer, lax.optimization_barrier(jnp.max(reached, axis=1)))
    decay_old = jnp.exp(boundary + stabilizer - new_stabilizer)
    shares = jnp.exp(reached - new_stabilizer[:, None, :])
    new_memory = decay_old[:, :, None, None] * memory + jnp.einsum('sjh,sjhv,sjhk->shvk', shares, value_all[:, :proposals], key_all[:, :proposals], precision=HIGHEST_PRECISION)
    new_normalizer = decay_old[:, :, None] * normalizer + jnp.einsum('sjh,sjhk->shk', shares, key_all[:, :proposals], precision=HIGHEST_PRECISION)
    return (cell_out, new_memory, new_normalizer, new_stabilizer)

def project(normed, weight):
    return jnp.dot(normed, weight.reshape(weight.shape[0], -1), preferred_element_type=jnp.float32)

def reference(tokens, norm_gain, w_query, w_key, w_value, w_outgate, w_input, w_forget, forget_bias, head_gain, w_out, memory, normalizer, stabilizer, prev_keys, prev_values, prev_input, prev_forget, accepted):
    sequences, proposals, model_width = tokens.shape
    heads = w_query.shape[1]
    key_size = w_query.shape[2]
    value_size = w_value.shape[2]
    as_float = tokens.astype(jnp.float32)
    inv_scale = lax.rsqrt(lax.optimization_barrier(jnp.mean(as_float * as_float, axis=-1, keepdims=True)) + EPS)
    normed = (as_float * inv_scale * norm_gain).astype(jnp.bfloat16).reshape(sequences * proposals, model_width)
    queries = project(normed, w_query).astype(jnp.bfloat16).reshape(sequences, proposals, heads, key_size)
    new_keys = project(normed, w_key).astype(jnp.bfloat16).reshape(sequences, proposals, heads, key_size)
    new_values = project(normed, w_value).astype(jnp.bfloat16).reshape(sequences, proposals, heads, value_size)
    out_gate = project(normed, w_outgate).reshape(sequences, proposals, heads, value_size)
    new_input = project(normed, w_input).reshape(sequences, proposals, heads)
    new_forget = jax.nn.log_sigmoid(project(normed, w_forget).reshape(sequences, proposals, heads) + forget_bias)
    query_f = queries.astype(jnp.float32) * key_size ** (-0.5)
    key_all = jnp.concatenate([prev_keys, new_keys], axis=1).astype(jnp.float32)
    value_all = jnp.concatenate([prev_values, new_values], axis=1).astype(jnp.float32)
    gate_in = jnp.concatenate([prev_input, new_input], axis=1)
    gate_forget = jnp.concatenate([prev_forget, new_forget], axis=1)
    cell_out, new_memory, new_normalizer, new_stabilizer = recurrent(query_f, key_all, value_all, gate_in, gate_forget, accepted, memory, normalizer, stabilizer)
    squares = lax.optimization_barrier(jnp.mean(cell_out * cell_out, axis=-1, keepdims=True))
    gated = (jax.nn.sigmoid(out_gate) * cell_out * lax.rsqrt(squares + EPS) * head_gain).astype(jnp.bfloat16)
    mixed = jnp.dot(gated.reshape(sequences * proposals, heads * value_size), w_out.reshape(heads * value_size, model_width), preferred_element_type=jnp.float32)
    mixed = mixed.astype(jnp.bfloat16).reshape(sequences, proposals, model_width)
    return (mixed, new_memory, new_normalizer, new_stabilizer, new_keys, new_values, new_input, new_forget)
```

```python
import functools

import jax
import jax.numpy as jnp
from jax import lax
from jax.experimental import pallas as pl
from jax.experimental.pallas import tpu as pltpu
from jax.sharding import PartitionSpec as P

EPS = 1e-06
FAR_NEGATIVE = -1e30
F32 = jnp.float32
BF16 = jnp.bfloat16
HIGHEST = lax.Precision.HIGHEST
PACK = 16


def iota(shape, dim):
    return lax.broadcasted_iota(jnp.int32, shape, dim)


def dot(a, b, precision=None):
    return jnp.dot(a, b, preferred_element_type=F32, precision=precision)


def dot_t(a, b, precision=None):
    return lax.dot_general(
        a, b, (((1,), (1,)), ((), ())), preferred_element_type=F32, precision=precision
    )


def log_sigmoid(x):
    return jnp.minimum(x, 0.0) - jnp.log1p(jnp.exp(-jnp.abs(x)))


def kept_gates(prev_in, prev_forget, accepted):
    dropped = iota(prev_in.shape, 0) >= accepted
    return jnp.where(dropped, FAR_NEGATIVE, prev_in), jnp.where(dropped, 0.0, prev_forget)


def running_rows(forget):
    rows = [forget[0:1]]
    for j in range(1, forget.shape[0]):
        rows.append(rows[-1] + forget[j : j + 1])
    return rows


def state_kernel(
    acc_ref, pi_ref, pf_ref, stab_ref, pk_ref, pv_ref, nrm_ref, mem_ref,
    new_mem_ref, new_nrm_ref, new_stab_ref, ks_ref, vt_ref, decay_ref,
):
    seqs, values, keys = mem_ref.shape
    steps = pi_ref.shape[0]
    rows = seqs * steps
    inflow, forget = kept_gates(pi_ref[...], pf_ref[...], acc_ref[...])
    running = running_rows(forget)
    edge = running[-1]
    stab = stab_ref[...]
    reached = [edge - running[j] + inflow[j : j + 1] for j in range(steps)]
    top = edge + stab
    for r in reached:
        top = jnp.maximum(top, r)
    new_stab_ref[...] = top
    decay = jnp.exp(edge + stab - top)
    row, lane = iota((rows, seqs), 0), iota((rows, seqs), 1)
    picked = jnp.zeros((rows, seqs), F32)
    for j in range(steps):
        picked = jnp.where(row == lane * steps + j, jnp.exp(reached[j] - top), picked)
    share_col = jnp.sum(picked, axis=1, keepdims=True)
    same = iota((seqs, seqs), 0) == iota((seqs, seqs), 1)
    decay_col = jnp.sum(jnp.where(same, decay, 0.0), axis=1, keepdims=True)
    decay_ref[...] = jnp.broadcast_to(decay_col, decay_ref.shape)
    scaled = pk_ref[...].astype(F32) * share_col
    ks_ref[...] = scaled.astype(BF16)
    vt_ref[...] = pv_ref[...].astype(F32).T.astype(BF16)
    member = (iota((seqs, rows), 1) // steps == iota((seqs, rows), 0)).astype(F32)
    new_nrm_ref[...] = decay_col * nrm_ref[...] + dot(member, scaled, HIGHEST)
    wide = 128 // steps
    group = 4
    owner = iota((values, 128), 1) // steps
    for half in range(seqs // wide):
        ks = ks_ref[half * 128 : (half + 1) * 128, :]

        def body(g, carry, half=half, ks=ks):
            vt = vt_ref[:, half * 128 : (half + 1) * 128]
            parts = [
                jnp.where(owner == g * group + i, vt, jnp.zeros_like(vt)) for i in range(group)
            ]
            added = dot(jnp.concatenate(parts, axis=0), ks)
            for i in range(group):
                s = half * wide + g * group + i
                new_mem_ref[s] = (
                    decay_ref[pl.ds(s, 1), :] * mem_ref[s]
                    + added[i * values : (i + 1) * values, :]
                )
            return carry

        lax.fori_loop(0, wide // group, body, 0)


def update_state(accepted, prev_in, prev_forget, stab, pk, pv, normalizer, memory):
    seqs, values, keys = memory.shape
    rows = pk.shape[0]
    return pl.pallas_call(
        state_kernel,
        name="state",
        out_shape=(
            jax.ShapeDtypeStruct(memory.shape, F32),
            jax.ShapeDtypeStruct(normalizer.shape, F32),
            jax.ShapeDtypeStruct(stab.shape, F32),
        ),
        scratch_shapes=[
            pltpu.VMEM((rows, keys), BF16),
            pltpu.VMEM((values, rows), BF16),
            pltpu.VMEM((seqs, keys), F32),
        ],
        cost_estimate=pl.CostEstimate(flops=200000000, bytes_accessed=4500000, transcendentals=400),
        compiler_params=pltpu.CompilerParams(vmem_limit_bytes=16 * 1024 * 1024),
    )(accepted, prev_in, prev_forget, stab, pk, pv, normalizer, memory)


def cell_kernel(
    ids_ref, xo_ref, xp_ref, rest_ref, gain_ref, wk_ref, wv_ref, wq_ref, wo_ref, wi_ref, wf_ref,
    bias_ref, hg_ref, acc_ref, pi_ref, pf_ref, stab_ref, pk_ref, pv_ref, nrm_ref, mem_ref,
    msg_ref, nk_ref, nv_ref, ni_ref, nf_ref, proj_ref, gate_ref, mq_ref,
):
    tp, head = ids_ref[0], ids_ref[1]
    blocks, main, lanes = xo_ref.shape
    seqs, values, keys = mem_ref.shape
    steps = pi_ref.shape[0]
    rows = seqs * steps
    heads = wi_ref.shape[0]
    width = gain_ref.shape[1]

    def tokens(z):
        top = jnp.concatenate([xo_ref[z], xp_ref[z]], axis=1)
        low = jnp.concatenate([rest_ref[2 * z + tp], rest_ref[2 * z + 1 - tp]], axis=1)
        return jnp.concatenate([top, low], axis=0).astype(F32)

    def square(z, total):
        x = tokens(z)
        x = x * x
        return total + (x[:, :lanes] + x[:, lanes:])

    total = lax.fori_loop(0, blocks, square, jnp.zeros((rows, lanes), F32))
    inv = lax.rsqrt(jnp.sum(total, axis=1, keepdims=True) / width + EPS)
    proj_ref[...] = jnp.zeros_like(proj_ref)
    gate_ref[...] = jnp.zeros_like(gate_ref)

    def project(z, carry):
        own = pl.ds(pl.multiple_of((2 * z + tp) * lanes, lanes), lanes)
        other = pl.ds(pl.multiple_of((2 * z + 1 - tp) * lanes, lanes), lanes)

        def both(ref):
            return jnp.concatenate([ref[:, own], ref[:, other]], axis=1)

        normed = (tokens(z) * inv * both(gain_ref)).astype(BF16)
        weight = jnp.concatenate([both(r) for r in (wk_ref, wv_ref, wq_ref, wo_ref)], axis=0)
        proj_ref[...] += dot_t(normed, weight)
        gates = jnp.concatenate([both(wi_ref), both(wf_ref)], axis=0)
        gate_ref[...] += dot_t(gates, normed)
        return carry

    lax.fori_loop(0, blocks, project, 0)

    gates = gate_ref[...]
    grow = iota(gates.shape, 0)
    gate_in = jnp.sum(jnp.where(grow == head, gates, 0.0), axis=0, keepdims=True)
    gate_forget = jnp.sum(jnp.where(grow == heads + head, gates, 0.0), axis=0, keepdims=True)
    shape = (2 * steps, rows)
    spread = jnp.where(iota(shape, 0) < steps, gate_in, gate_forget)
    spread = jnp.where(iota(shape, 1) % steps == iota(shape, 0) % steps, spread, 0.0)
    member = (iota((rows, seqs), 0) // steps == iota((rows, seqs), 1)).astype(F32)
    compact = dot(spread, member, HIGHEST)
    bias = bias_ref[...]
    bias = jnp.sum(jnp.where(iota(bias.shape, 1) == head, bias, 0.0), axis=1, keepdims=True)
    new_in = compact[:steps]
    new_forget = log_sigmoid(compact[steps:] + bias)
    ni_ref[...] = new_in
    nf_ref[...] = new_forget
    old_in, old_forget = kept_gates(pi_ref[...], pf_ref[...], acc_ref[...])
    inflow = jnp.concatenate([old_in, new_in], axis=0)
    run = running_rows(jnp.concatenate([old_forget, new_forget], axis=0))
    running = jnp.concatenate(run, axis=0)
    stab = stab_ref[...]
    span = 2 * steps
    place = iota((span, seqs), 0)
    erow = iota((rows, seqs), 0)
    ecol = iota((rows, seqs), 1)
    coef = jnp.zeros((rows, 2 * span), F32)
    for t in range(steps):
        latest = run[steps + t]
        d = latest - running + inflow
        d = jnp.where(place <= steps + t, d, FAR_NEGATIVE)
        carried = latest + stab
        top = jnp.maximum(jnp.max(d, axis=0, keepdims=True), carried)
        weight = jnp.exp(d - top)
        tail = jnp.where(place == 0, jnp.exp(carried - top), jnp.exp(-top))
        stacked = jnp.concatenate([weight, tail], axis=0)
        pick = (erow == ecol * steps + t).astype(F32)
        coef = coef + dot_t(pick, stacked, HIGHEST)
    carry_scale = coef[:, span : span + 1]
    least = coef[:, span + 1 : span + 2]

    proj = proj_ref[...]
    new_k = proj[:, :keys].astype(BF16)
    new_v = proj[:, keys : keys + values].astype(BF16)
    nk_ref[...] = new_k
    nv_ref[...] = new_v
    query = proj[:, keys + values : 2 * keys + values].astype(BF16)
    query_f = query.astype(F32) * keys ** (-0.5)
    out_gate = proj[:, 2 * keys + values :]
    query_wide = jnp.concatenate([query_f, jnp.zeros((rows, values), F32)], axis=1)
    pair = keys + values
    known = jnp.concatenate(
        [pk_ref[...].astype(F32), pv_ref[...].astype(F32), proj[:, :pair]], axis=1
    ).astype(BF16)
    prow, plane = iota((rows, rows), 0), iota((rows, rows), 1)
    numerator = jnp.zeros((rows, pair), F32)
    denominator = jnp.zeros((rows, 1), F32)
    for u in range(steps):
        at = (plane == prow // steps * steps + u).astype(F32).astype(BF16)
        here = dot(at, known)
        for part, c in ((here[:, :pair], u), (here[:, pair:], steps + u)):
            score = jnp.sum(query_wide * part, axis=1, keepdims=True)
            w = coef[:, c : c + 1] * score
            numerator = numerator + w * part
            denominator = denominator + w

    group = 4
    span_rows = group * steps
    quarter = iota((span_rows, 2 * values), 0) // steps
    for g in range(seqs // group):
        block = mem_ref[g * group : (g + 1) * group].reshape(group * values, keys).astype(BF16)
        full = dot_t(query[g * span_rows : (g + 1) * span_rows, :], block)
        side = jnp.where(quarter < 2, full[:, : 2 * values], full[:, 2 * values :])
        mq_ref[g * span_rows : (g + 1) * span_rows, :] = jnp.where(
            quarter[:, :values] % 2 == 0, side[:, :values], side[:, values:]
        )
    norm_rows = dot(member, nrm_ref[...], HIGHEST)
    denominator = denominator + carry_scale * jnp.sum(query_f * norm_rows, axis=1, keepdims=True)
    numerator = numerator[:, keys:] + carry_scale * (mq_ref[...] * keys ** (-0.5))
    cell = numerator / jnp.maximum(jnp.abs(denominator), least)
    squares = dot_t(jnp.ones((8, values), F32), cell * cell, HIGHEST)[0:1]
    full_gain = hg_ref[...]
    gain = jnp.sum(jnp.where(iota(full_gain.shape, 0) == head, full_gain, 0.0), axis=0, keepdims=True)
    gain = jnp.where(tp == 0, gain[:, :values], gain[:, values:])
    gated = jax.nn.sigmoid(out_gate) * cell * gain
    half = rows // 2
    msg_ref[:half, :] = jnp.concatenate([gated[:half], gated[half:]], axis=1).astype(BF16)
    high = squares.astype(BF16).astype(F32)
    low = squares - high
    at = iota((PACK, half), 0)
    slab = jnp.where(at == 0, high[:, :half], 0.0)
    slab = jnp.where(at == 1, high[:, half:], slab)
    slab = jnp.where(at == 8, low[:, :half], slab)
    slab = jnp.where(at == 9, low[:, half:], slab)
    msg_ref[half:, :] = slab.astype(BF16)


def run_cell(*args):
    ids, xo = args[0], args[1]
    pi, pk, pv = args[14], args[17], args[18]
    rows, keys = pk.shape
    values = pv.shape[1]
    heads = args[9].shape[0]
    whole = [pl.BlockSpec(memory_space=pltpu.VMEM)] * (len(args) - 1)
    return pl.pallas_call(
        cell_kernel,
        name="cell",
        out_shape=(
            jax.ShapeDtypeStruct((rows // 2 + PACK, 2 * values), BF16),
            jax.ShapeDtypeStruct((rows, keys), BF16),
            jax.ShapeDtypeStruct((rows, values), BF16),
            jax.ShapeDtypeStruct(pi.shape, F32),
            jax.ShapeDtypeStruct(pi.shape, F32),
        ),
        in_specs=[pl.BlockSpec(memory_space=pltpu.SMEM)] + whole,
        scratch_shapes=[
            pltpu.VMEM((rows, 2 * keys + 2 * values), F32),
            pltpu.VMEM((2 * heads, rows), F32),
            pltpu.VMEM((rows, values), F32),
        ],
        cost_estimate=pl.CostEstimate(flops=1500000000, bytes_accessed=8000000, transcendentals=100000),
        compiler_params=pltpu.CompilerParams(vmem_limit_bytes=32 * 1024 * 1024),
    )(*args)


def out_kernel(ids_ref, own_ref, other_ref, w_ref, out_ref):
    tp = ids_ref[0]
    heads, tall, lanes = own_ref.shape
    half = tall - PACK
    parts, _, chunk, feats = w_ref.shape
    values = parts * chunk
    slab = own_ref[:, half:, :].astype(F32) + other_ref[:, half:, :].astype(F32)
    squares = (slab[:, :8, :] + slab[:, 8:, :]).reshape(heads * 8, half)
    inv = lax.rsqrt(squares / (2 * values) + EPS).T
    zero = jnp.zeros((values, feats), BF16)
    low = jnp.zeros((half, feats), F32)
    high = jnp.zeros((half, feats), F32)
    for h in range(heads):
        sent = jnp.concatenate([own_ref[h, :half, :], other_ref[h, :half, :]], axis=1)
        mine = jnp.concatenate([w_ref[d, 2 * h + tp] for d in range(parts)], axis=0)
        theirs = jnp.concatenate([w_ref[d, 2 * h + 1 - tp] for d in range(parts)], axis=0)
        weight = jnp.concatenate(
            [
                jnp.concatenate([mine, zero, theirs, zero], axis=0),
                jnp.concatenate([zero, mine, zero, theirs], axis=0),
            ],
            axis=1,
        )
        both = dot(sent, weight)
        low = low + inv[:, 8 * h : 8 * h + 1] * both[:, :feats]
        high = high + inv[:, 8 * h + 1 : 8 * h + 2] * both[:, feats:]
    out_ref[:half, :] = low.astype(BF16)
    out_ref[half:, :] = high.astype(BF16)


def project_out(ids, own, other, weight):
    rows = 2 * (own.shape[1] - PACK)
    return pl.pallas_call(
        out_kernel,
        name="mix",
        out_shape=jax.ShapeDtypeStruct((rows, weight.shape[3]), BF16),
        in_specs=[pl.BlockSpec(memory_space=pltpu.SMEM)] + [pl.BlockSpec(memory_space=pltpu.VMEM)] * 3,
        cost_estimate=pl.CostEstimate(flops=270000000, bytes_accessed=2000000, transcendentals=10000),
        compiler_params=pltpu.CompilerParams(vmem_limit_bytes=16 * 1024 * 1024),
    )(ids, own, other, weight)


def swap(value, axis):
    size = lax.axis_size(axis)
    return lax.ppermute(value, axis, [(i, size - 1 - i) for i in range(size)])


def shards(
    tokens,
    norm_gain,
    w_query,
    w_key,
    w_value,
    w_outgate,
    w_input,
    w_forget,
    forget_bias,
    head_gain,
    w_out,
    memory,
    normalizer,
    stabilizer,
    prev_keys,
    prev_values,
    prev_input,
    prev_forget,
    accepted,
):
    seqs, steps, lanes = tokens.shape
    rows = seqs * steps
    keys, values = w_query.shape[2], w_value.shape[2]
    kv, tp, dp = lax.axis_size("kv"), lax.axis_size("tp"), lax.axis_size("dp")
    ids = jnp.stack([lax.axis_index("tp"), lax.axis_index("kv")]).astype(jnp.int32)
    x = tokens.reshape(rows, lanes)
    main = rows - PACK
    chunk = values // dp

    piece = lax.dynamic_slice_in_dim(w_out[0], lax.axis_index("dp") * chunk, chunk, 0)
    piece = piece.reshape(chunk, kv * tp, lanes).transpose(1, 0, 2)
    last = jnp.broadcast_to(x[main:][None], (kv * tp, PACK, lanes))
    first = lax.all_to_all(
        jnp.concatenate([last, piece], axis=1), ("kv", "tp"), 0, 0, tiled=True
    )
    own = lax.all_gather(x[:main], "kv")
    other = swap(own, "tp")
    rest = first[:, :PACK]
    piece = first[:, PACK:]
    weight = lax.all_to_all(
        jnp.broadcast_to(piece[None], (dp, *piece.shape)), "dp", 0, 0, tiled=True
    )

    def turned(w):
        return w.transpose(1, 2, 0).reshape(-1, w.shape[0])

    acc = accepted.reshape(1, seqs)
    pi = prev_input.transpose(1, 2, 0).reshape(steps, seqs)
    pf = prev_forget.transpose(1, 2, 0).reshape(steps, seqs)
    stab = stabilizer.transpose(1, 0)
    pk = prev_keys.reshape(rows, keys)
    pv = prev_values.reshape(rows, values)
    nrm = normalizer.reshape(seqs, keys)
    mem = memory.reshape(seqs, values, keys)
    new_memory, new_normalizer, new_stabilizer = update_state(acc, pi, pf, stab, pk, pv, nrm, mem)
    msg, new_keys, new_values, new_input, new_forget = run_cell(
        ids, own, other, rest, norm_gain.reshape(1, -1),
        turned(w_key), turned(w_value), turned(w_query), turned(w_outgate), w_input.T, w_forget.T,
        forget_bias.reshape(1, -1), head_gain, acc, pi, pf, stab, pk, pv, nrm, mem,
    )
    gated = lax.all_gather(msg, "kv")
    mixed = project_out(ids, gated, swap(gated, "tp"), weight)
    return (
        mixed.reshape(seqs, steps, lanes),
        new_memory.reshape(memory.shape),
        new_normalizer.reshape(normalizer.shape),
        new_stabilizer.transpose(1, 0),
        new_keys.reshape(prev_keys.shape),
        new_values.reshape(prev_values.shape),
        new_input.reshape(steps, 1, seqs).transpose(2, 0, 1),
        new_forget.reshape(steps, 1, seqs).transpose(2, 0, 1),
    )


def solution(mesh):
    specs = (
        P(("grp", "dp"), None, ("kv", "tp")),
        P(),
        P(None, "kv", None),
        P(None, "kv", None),
        P(None, "kv", "tp"),
        P(None, "kv", "tp"),
        P(),
        P(),
        P(),
        P(),
        P("kv", "tp", None),
        P(("grp", "dp"), "kv", "tp", None),
        P(("grp", "dp"), "kv", None),
        P(("grp", "dp"), "kv"),
        P(("grp", "dp"), None, "kv", None),
        P(("grp", "dp"), None, "kv", "tp"),
        P(("grp", "dp"), None, "kv"),
        P(("grp", "dp"), None, "kv"),
        P(("grp", "dp")),
    )
    outs = (
        P(("grp", "dp"), None, ("kv", "tp")),
        P(("grp", "dp"), "kv", "tp", None),
        P(("grp", "dp"), "kv", None),
        P(("grp", "dp"), "kv"),
        P(("grp", "dp"), None, "kv", None),
        P(("grp", "dp"), None, "kv", "tp"),
        P(("grp", "dp"), None, "kv"),
        P(("grp", "dp"), None, "kv"),
    )
    return jax.shard_map(shards, mesh=mesh, in_specs=specs, out_specs=outs, check_vma=False)
```

```python
import jax
import jax.numpy as jnp
from jax import lax
from jax.experimental import pallas as pl
from jax.experimental.pallas import tpu as pltpu
from jax.sharding import PartitionSpec as P


EPS = 1e-06
FAR_NEGATIVE = -1e30
F32 = jnp.float32
BF16 = jnp.bfloat16
HIGHEST = lax.Precision.HIGHEST
NEAR = 4
CUTS = 2
PACK = 16


def iota(shape, dim):
    return lax.broadcasted_iota(jnp.int32, shape, dim)


def dot(a, b, precision=None):
    return jnp.dot(a, b, preferred_element_type=F32, precision=precision)


def dot_t(a, b, precision=None):
    return lax.dot_general(
        a, b, (((1,), (1,)), ((), ())), preferred_element_type=F32, precision=precision
    )


def log_sigmoid(x):
    return jnp.minimum(x, 0.0) - jnp.log1p(jnp.exp(-jnp.abs(x)))


def kept_gates(prev_in, prev_forget, accepted):
    dropped = iota(prev_in.shape, 0) >= accepted
    return jnp.where(dropped, FAR_NEGATIVE, prev_in), jnp.where(dropped, 0.0, prev_forget)


def running_rows(forget):
    rows = [forget[0:1]]
    for j in range(1, forget.shape[0]):
        rows.append(rows[-1] + forget[j : j + 1])
    return rows


def state_kernel(
    acc_ref, pi_ref, pf_ref, stab_ref, pk_ref, pv_ref, nrm_ref, mem_ref,
    new_mem_ref, new_nrm_ref, new_stab_ref, ks_ref, vt_ref, decay_ref,
):
    seqs, values, _ = mem_ref.shape
    steps = pi_ref.shape[0]
    rows = seqs * steps
    inflow, forget = kept_gates(pi_ref[...], pf_ref[...], acc_ref[...])
    running = running_rows(forget)
    edge = running[-1]
    stab = stab_ref[...]
    reached = [edge - running[j] + inflow[j : j + 1] for j in range(steps)]
    top = edge + stab
    for r in reached:
        top = jnp.maximum(top, r)
    new_stab_ref[...] = top
    decay = jnp.exp(edge + stab - top)
    row, lane = iota((rows, seqs), 0), iota((rows, seqs), 1)
    picked = jnp.zeros((rows, seqs), F32)
    for j in range(steps):
        picked = jnp.where(row == lane * steps + j, jnp.exp(reached[j] - top), picked)
    share_col = jnp.sum(picked, axis=1, keepdims=True)
    same = iota((seqs, seqs), 0) == iota((seqs, seqs), 1)
    decay_col = jnp.sum(jnp.where(same, decay, 0.0), axis=1, keepdims=True)
    decay_ref[...] = jnp.broadcast_to(decay_col, decay_ref.shape)
    scaled = pk_ref[...].astype(F32) * share_col
    ks_ref[...] = scaled.astype(BF16)
    vt_ref[...] = pv_ref[...].astype(F32).T.astype(BF16)
    member = (iota((seqs, rows), 1) // steps == iota((seqs, rows), 0)).astype(F32)
    new_nrm_ref[...] = decay_col * nrm_ref[...] + dot(member, scaled, HIGHEST)
    wide = 128 // steps
    group = 4
    owner = iota((values, 128), 1) // steps
    for half in range(seqs // wide):
        ks = ks_ref[half * 128 : (half + 1) * 128, :]

        def body(g, carry, half=half, ks=ks):
            vt = vt_ref[:, half * 128 : (half + 1) * 128]
            parts = [
                jnp.where(owner == g * group + i, vt, jnp.zeros_like(vt)) for i in range(group)
            ]
            added = dot(jnp.concatenate(parts, axis=0), ks)
            for i in range(group):
                s = half * wide + g * group + i
                new_mem_ref[s] = (
                    decay_ref[pl.ds(s, 1), :] * mem_ref[s]
                    + added[i * values : (i + 1) * values, :]
                )
            return carry

        lax.fori_loop(0, wide // group, body, 0)


def update_state(accepted, prev_in, prev_forget, stab, pk, pv, normalizer, memory):
    seqs, values, keys = memory.shape
    rows = pk.shape[0]
    return pl.pallas_call(
        state_kernel,
        name="state",
        out_shape=(
            jax.ShapeDtypeStruct(memory.shape, F32),
            jax.ShapeDtypeStruct(normalizer.shape, F32),
            jax.ShapeDtypeStruct(stab.shape, F32),
        ),
        scratch_shapes=[
            pltpu.VMEM((rows, keys), BF16),
            pltpu.VMEM((values, rows), BF16),
            pltpu.VMEM((seqs, keys), F32),
        ],
        cost_estimate=pl.CostEstimate(flops=200000000, bytes_accessed=4500000, transcendentals=400),
        compiler_params=pltpu.CompilerParams(vmem_limit_bytes=8 * 1024 * 1024),
    )(accepted, prev_in, prev_forget, stab, pk, pv, normalizer, memory)


def cell_kernel(
    ids_ref, xo_hbm, xp_hbm, gain_ref, wk_hbm, wv_hbm, wq_hbm, wo_hbm, wi_hbm, wf_hbm,
    bias_ref, hg_ref, acc_ref, pi_ref, pf_ref, stab_ref, pk_ref, pv_ref, nrm_ref, mem_hbm,
    msg_ref, nk_ref, nv_ref, ni_ref, nf_ref, xo_ref, xp_ref, w_ref, wg_ref, mem_ref, normed_ref,
    mq_ref, token_sem, weight_sem,
):
    tp, head = ids_ref[0], ids_ref[1]
    blocks, _, lanes = xo_ref.shape
    seqs, values, keys = mem_ref.shape
    steps = pi_ref.shape[0]
    rows = seqs * steps
    heads = wg_ref.shape[0] // 2
    width = gain_ref.shape[1]
    half = blocks // CUTS
    arriving = []
    for i in range(CUTS):
        part = pl.ds(i * half, half)
        for n, (src, dst) in enumerate(((xo_hbm, xo_ref), (xp_hbm, xp_ref))):
            arriving.append(pltpu.make_async_copy(src.at[part], dst.at[part], token_sem.at[i, n]))
    loads = [
        pltpu.make_async_copy(src, w_ref.at[pl.ds(i * keys, keys)], weight_sem.at[i])
        for i, src in enumerate((wk_hbm, wv_hbm, wq_hbm, wo_hbm))
    ]
    loads.append(pltpu.make_async_copy(wi_hbm, wg_ref.at[pl.ds(0, heads)], weight_sem.at[4]))
    loads.append(pltpu.make_async_copy(wf_hbm, wg_ref.at[pl.ds(heads, heads)], weight_sem.at[5]))
    state_load = pltpu.make_async_copy(mem_hbm, mem_ref, weight_sem.at[6])
    for copy in (*arriving, *loads, state_load):
        copy.start()

    def square(z, total):
        a, b = xo_ref[z].astype(F32), xp_ref[z].astype(F32)
        return total + (a * a + b * b)

    total = jnp.zeros((rows, lanes), F32)
    for i in range(CUTS):
        arriving[2 * i].wait()
        arriving[2 * i + 1].wait()
        total = lax.fori_loop(i * half, (i + 1) * half, square, total)
    inv = lax.rsqrt(jnp.sum(total, axis=1, keepdims=True) / width + EPS)
    inv = jnp.broadcast_to(inv, (rows, lanes))

    def normalize(p, carry):
        z = p % (blocks // NEAR) * NEAR + p // (blocks // NEAR)
        for ref, side in ((xo_ref, tp), (xp_ref, 1 - tp)):
            at = pl.ds(pl.multiple_of((2 * z + side) * lanes, lanes), lanes)
            normed_ref[:, at] = (ref[p].astype(F32) * inv * gain_ref[:, at]).astype(BF16)
        return carry

    lax.fori_loop(0, blocks, normalize, 0)
    for copy in loads:
        copy.wait()
    normed = normed_ref[...]
    proj = dot_t(normed, w_ref[...])
    gates = dot_t(wg_ref[...], normed)

    grow = iota(gates.shape, 0)
    gate_in = jnp.sum(jnp.where(grow == head, gates, 0.0), axis=0, keepdims=True)
    gate_forget = jnp.sum(jnp.where(grow == heads + head, gates, 0.0), axis=0, keepdims=True)
    shape = (2 * steps, rows)
    spread = jnp.where(iota(shape, 0) < steps, gate_in, gate_forget)
    spread = jnp.where(iota(shape, 1) % steps == iota(shape, 0) % steps, spread, 0.0)
    member = (iota((rows, seqs), 0) // steps == iota((rows, seqs), 1)).astype(F32)
    compact = dot(spread, member, HIGHEST)
    bias = bias_ref[...]
    bias = jnp.sum(jnp.where(iota(bias.shape, 1) == head, bias, 0.0), axis=1, keepdims=True)
    new_in = compact[:steps]
    new_forget = log_sigmoid(compact[steps:] + bias)
    ni_ref[...] = new_in
    nf_ref[...] = new_forget
    old_in, old_forget = kept_gates(pi_ref[...], pf_ref[...], acc_ref[...])
    inflow = jnp.concatenate([old_in, new_in], axis=0)
    run = running_rows(jnp.concatenate([old_forget, new_forget], axis=0))
    running = jnp.concatenate(run, axis=0)
    stab = stab_ref[...]
    span = 2 * steps
    place = iota((span, seqs), 0)
    erow = iota((rows, seqs), 0)
    ecol = iota((rows, seqs), 1)
    coef = jnp.zeros((rows, 2 * span), F32)
    for t in range(steps):
        latest = run[steps + t]
        d = latest - running + inflow
        d = jnp.where(place <= steps + t, d, FAR_NEGATIVE)
        carried = latest + stab
        top = jnp.maximum(jnp.max(d, axis=0, keepdims=True), carried)
        weight = jnp.exp(d - top)
        tail = jnp.where(place == 0, jnp.exp(carried - top), jnp.exp(-top))
        stacked = jnp.concatenate([weight, tail], axis=0)
        pick = (erow == ecol * steps + t).astype(F32)
        coef = coef + dot_t(pick, stacked, HIGHEST)
    carry_scale = coef[:, span : span + 1]
    least = coef[:, span + 1 : span + 2]

    new_k = proj[:, :keys].astype(BF16)
    new_v = proj[:, keys : keys + values].astype(BF16)
    nk_ref[...] = new_k
    nv_ref[...] = new_v
    query = proj[:, keys + values : 2 * keys + values].astype(BF16)
    query_f = query.astype(F32) * keys ** (-0.5)
    out_gate = proj[:, 2 * keys + values :]
    query_wide = jnp.concatenate([query_f, jnp.zeros((rows, values), F32)], axis=1)
    pair = keys + values
    known = jnp.concatenate(
        [pk_ref[...].astype(F32), pv_ref[...].astype(F32), proj[:, :pair]], axis=1
    ).astype(BF16)
    prow, plane = iota((rows, rows), 0), iota((rows, rows), 1)
    numerator = jnp.zeros((rows, pair), F32)
    denominator = jnp.zeros((rows, 1), F32)
    for u in range(steps):
        at = (plane == prow // steps * steps + u).astype(F32).astype(BF16)
        here = dot(at, known)
        for part, c in ((here[:, :pair], u), (here[:, pair:], steps + u)):
            score = jnp.sum(query_wide * part, axis=1, keepdims=True)
            w = coef[:, c : c + 1] * score
            numerator = numerator + w * part
            denominator = denominator + w

    state_load.wait()
    group = 4
    span_rows = group * steps
    quarter = iota((span_rows, 2 * values), 0) // steps
    for g in range(seqs // group):
        block = mem_ref[g * group : (g + 1) * group].reshape(group * values, keys).astype(BF16)
        full = dot_t(query[g * span_rows : (g + 1) * span_rows, :], block)
        side = jnp.where(quarter < 2, full[:, : 2 * values], full[:, 2 * values :])
        mq_ref[g * span_rows : (g + 1) * span_rows, :] = jnp.where(
            quarter[:, :values] % 2 == 0, side[:, :values], side[:, values:]
        )
    norm_rows = dot(member, nrm_ref[...], HIGHEST)
    denominator = denominator + carry_scale * jnp.sum(query_f * norm_rows, axis=1, keepdims=True)
    numerator = numerator[:, keys:] + carry_scale * (mq_ref[...] * keys ** (-0.5))
    cell = numerator / jnp.maximum(jnp.abs(denominator), least)
    squares = dot_t(jnp.ones((8, values), F32), cell * cell, HIGHEST)[0:1]
    full_gain = hg_ref[...]
    gain = jnp.sum(jnp.where(iota(full_gain.shape, 0) == head, full_gain, 0.0), axis=0, keepdims=True)
    gain = jnp.where(tp == 0, gain[:, :values], gain[:, values:])
    gated = jax.nn.sigmoid(out_gate) * cell * gain
    half = rows // 2
    msg_ref[:half, :] = jnp.concatenate([gated[:half], gated[half:]], axis=1).astype(BF16)
    high = squares.astype(BF16).astype(F32)
    low = squares - high
    at = iota((PACK, half), 0)
    slab = jnp.where(at == 0, high[:, :half], 0.0)
    slab = jnp.where(at == 1, high[:, half:], slab)
    slab = jnp.where(at == 8, low[:, :half], slab)
    slab = jnp.where(at == 9, low[:, half:], slab)
    msg_ref[half:, :] = slab.astype(BF16)


def run_cell(*args):
    xo = args[1]
    pi, pk, pv = args[13], args[16], args[17]
    rows, keys = pk.shape
    values = pv.shape[1]
    heads = args[8].shape[0]
    seqs, width = args[18].shape[0], args[3].shape[1]
    space = {i: pltpu.HBM for i in (4, 5, 6, 7, 8, 9, 19)}
    space.update({i: pl.ANY for i in (1, 2)})
    whole = [
        pl.BlockSpec(memory_space=space.get(i, pltpu.VMEM)) for i in range(1, len(args))
    ]
    return pl.pallas_call(
        cell_kernel,
        name="cell",
        out_shape=(
            jax.ShapeDtypeStruct((rows // 2 + PACK, 2 * values), BF16),
            jax.ShapeDtypeStruct((rows, keys), BF16),
            jax.ShapeDtypeStruct((rows, values), BF16),
            jax.ShapeDtypeStruct(pi.shape, F32),
            jax.ShapeDtypeStruct(pi.shape, F32),
        ),
        in_specs=[pl.BlockSpec(memory_space=pltpu.SMEM)] + whole,
        scratch_shapes=[
            pltpu.VMEM(xo.shape, BF16),
            pltpu.VMEM(xo.shape, BF16),
            pltpu.VMEM((2 * keys + 2 * values, width), BF16),
            pltpu.VMEM((2 * heads, width), BF16),
            pltpu.VMEM((seqs, values, keys), F32),
            pltpu.VMEM((rows, width), BF16),
            pltpu.VMEM((rows, values), F32),
            pltpu.SemaphoreType.DMA((CUTS, 2)),
            pltpu.SemaphoreType.DMA((7,)),
        ],
        cost_estimate=pl.CostEstimate(flops=1500000000, bytes_accessed=8000000, transcendentals=100000),
        compiler_params=pltpu.CompilerParams(vmem_limit_bytes=56 * 1024 * 1024),
    )(*args)


def out_kernel(ids_ref, own_hbm, other_hbm, w_hbm, out_ref, own_ref, other_ref, w_ref, sem):
    tp = ids_ref[0]
    heads, tall, _ = own_ref.shape
    half = tall - PACK
    parts, _, chunk, feats = w_ref.shape
    values = parts * chunk
    copies = [
        pltpu.make_async_copy(src, dst, sem.at[i])
        for i, (src, dst) in enumerate(
            ((own_hbm, own_ref), (other_hbm, other_ref), (w_hbm, w_ref))
        )
    ]
    for copy in copies:
        copy.start()
    for copy in copies:
        copy.wait()
    slab = own_ref[:, half:, :].astype(F32) + other_ref[:, half:, :].astype(F32)
    squares = (slab[:, :8, :] + slab[:, 8:, :]).reshape(heads * 8, half)
    inv = lax.rsqrt(squares / (2 * values) + EPS).T
    zero = jnp.zeros((values, feats), BF16)
    low = jnp.zeros((half, feats), F32)
    high = jnp.zeros((half, feats), F32)
    for h in range(heads):
        sent = jnp.concatenate([own_ref[h, :half, :], other_ref[h, :half, :]], axis=1)
        mine = jnp.concatenate([w_ref[d, 2 * h + tp] for d in range(parts)], axis=0)
        theirs = jnp.concatenate([w_ref[d, 2 * h + 1 - tp] for d in range(parts)], axis=0)
        weight = jnp.concatenate(
            [
                jnp.concatenate([mine, zero, theirs, zero], axis=0),
                jnp.concatenate([zero, mine, zero, theirs], axis=0),
            ],
            axis=1,
        )
        both = dot(sent, weight)
        low = low + inv[:, 8 * h : 8 * h + 1] * both[:, :feats]
        high = high + inv[:, 8 * h + 1 : 8 * h + 2] * both[:, feats:]
    out_ref[:half, :] = low.astype(BF16)
    out_ref[half:, :] = high.astype(BF16)


def project_out(ids, own, other, weight):
    rows = 2 * (own.shape[1] - PACK)
    return pl.pallas_call(
        out_kernel,
        name="mix",
        out_shape=jax.ShapeDtypeStruct((rows, weight.shape[3]), BF16),
        in_specs=[pl.BlockSpec(memory_space=pltpu.SMEM)] + [pl.BlockSpec(memory_space=pl.ANY)] * 3,
        scratch_shapes=[
            pltpu.VMEM(own.shape, BF16),
            pltpu.VMEM(own.shape, BF16),
            pltpu.VMEM(weight.shape, BF16),
            pltpu.SemaphoreType.DMA((3,)),
        ],
        cost_estimate=pl.CostEstimate(flops=270000000, bytes_accessed=2000000, transcendentals=10000),
        compiler_params=pltpu.CompilerParams(vmem_limit_bytes=8 * 1024 * 1024),
    )(ids, own, other, weight)


def swap(value, axis):
    size = lax.axis_size(axis)
    return lax.ppermute(value, axis, [(i, size - 1 - i) for i in range(size)])


def copies(value, count):
    return jnp.broadcast_to(value[None], (count, *value.shape))


def shards(
    tokens,
    norm_gain,
    w_query,
    w_key,
    w_value,
    w_outgate,
    w_input,
    w_forget,
    forget_bias,
    head_gain,
    w_out,
    memory,
    normalizer,
    stabilizer,
    prev_keys,
    prev_values,
    prev_input,
    prev_forget,
    accepted,
):
    seqs, steps, lanes = tokens.shape
    rows = seqs * steps
    keys, values = w_query.shape[2], w_value.shape[2]
    kv, tp = lax.axis_size("kv"), lax.axis_size("tp")
    ids = jnp.stack([lax.axis_index("tp"), lax.axis_index("kv")]).astype(jnp.int32)
    x = tokens.reshape(rows, lanes)

    far = kv // NEAR
    apart = [[q + NEAR * i for i in range(far)] for q in range(NEAR)]
    beside = [[NEAR * i + q for q in range(NEAR)] for i in range(far)]
    own = lax.all_to_all(
        copies(x, far), "kv", 0, 0, tiled=True, axis_index_groups=apart
    )
    own = lax.all_to_all(
        copies(own, NEAR), "kv", 0, 0, tiled=True, axis_index_groups=beside
    )
    own = own.reshape(kv, rows, lanes)
    other = swap(own, "tp")

    piece = w_out[0].reshape(values, kv * tp, lanes).transpose(1, 0, 2)
    weight = lax.all_to_all(piece, ("kv", "tp"), 0, 0, tiled=True)[None]

    def turned(w):
        return w.transpose(1, 2, 0).reshape(-1, w.shape[0])

    acc = accepted.reshape(1, seqs)
    pi = prev_input.transpose(1, 2, 0).reshape(steps, seqs)
    pf = prev_forget.transpose(1, 2, 0).reshape(steps, seqs)
    stab = stabilizer.transpose(1, 0)
    pk = prev_keys.reshape(rows, keys)
    pv = prev_values.reshape(rows, values)
    nrm = normalizer.reshape(seqs, keys)
    mem = memory.reshape(seqs, values, keys)
    new_memory, new_normalizer, new_stabilizer = update_state(acc, pi, pf, stab, pk, pv, nrm, mem)
    msg, new_keys, new_values, new_input, new_forget = run_cell(
        ids, own, other, norm_gain.reshape(1, -1),
        turned(w_key), turned(w_value), turned(w_query), turned(w_outgate), w_input.T, w_forget.T,
        forget_bias.reshape(1, -1), head_gain, acc, pi, pf, stab, pk, pv, nrm, mem,
    )
    gated = lax.all_gather(msg, "kv")
    mixed = project_out(ids, gated, swap(gated, "tp"), weight)
    return (
        mixed.reshape(seqs, steps, lanes),
        new_memory.reshape(memory.shape),
        new_normalizer.reshape(normalizer.shape),
        new_stabilizer.transpose(1, 0),
        new_keys.reshape(prev_keys.shape),
        new_values.reshape(prev_values.shape),
        new_input.reshape(steps, 1, seqs).transpose(2, 0, 1),
        new_forget.reshape(steps, 1, seqs).transpose(2, 0, 1),
    )


def solution(mesh):
    specs = (
        P(("grp", "dp"), None, ("kv", "tp")),
        P(),
        P(None, "kv", None),
        P(None, "kv", None),
        P(None, "kv", "tp"),
        P(None, "kv", "tp"),
        P(),
        P(),
        P(),
        P(),
        P("kv", "tp", None),
        P(("grp", "dp"), "kv", "tp", None),
        P(("grp", "dp"), "kv", None),
        P(("grp", "dp"), "kv"),
        P(("grp", "dp"), None, "kv", None),
        P(("grp", "dp"), None, "kv", "tp"),
        P(("grp", "dp"), None, "kv"),
        P(("grp", "dp"), None, "kv"),
        P(("grp", "dp")),
    )
    outs = (
        P(("grp", "dp"), None, ("kv", "tp")),
        P(("grp", "dp"), "kv", "tp", None),
        P(("grp", "dp"), "kv", None),
        P(("grp", "dp"), "kv"),
        P(("grp", "dp"), None, "kv", None),
        P(("grp", "dp"), None, "kv", "tp"),
        P(("grp", "dp"), None, "kv"),
        P(("grp", "dp"), None, "kv"),
    )

    return jax.shard_map(shards, mesh=mesh, in_specs=specs, out_specs=outs, check_vma=False)
```

```python
import jax
import jax.numpy as jnp
from jax import lax
from jax.experimental import pallas as pl
from jax.experimental.pallas import tpu as pltpu
from jax.sharding import PartitionSpec as P


EPS = 1e-06
FAR_NEGATIVE = -1e30
F32 = jnp.float32
BF16 = jnp.bfloat16
STATE_CUTS = 4
CUTS = 4
LAST = 8
PACK = 16


def iota(shape, dim):
    return lax.broadcasted_iota(jnp.int32, shape, dim)


def dot(a, b, precision=None):
    return jnp.dot(a, b, preferred_element_type=F32, precision=precision)


def dot_t(a, b, precision=None):
    return lax.dot_general(
        a, b, (((1,), (1,)), ((), ())), preferred_element_type=F32, precision=precision
    )


def split(x, parts):
    pieces = []
    for _ in range(parts):
        piece = x.astype(BF16)
        pieces.append(piece)
        x = x - piece.astype(F32)
    return pieces


def log_sigmoid(x):
    return jnp.minimum(x, 0.0) - jnp.log1p(jnp.exp(-jnp.abs(x)))


def kept_gates(prev_in, prev_forget, accepted):
    dropped = iota(prev_in.shape, 0) >= accepted
    return jnp.where(dropped, FAR_NEGATIVE, prev_in), jnp.where(dropped, 0.0, prev_forget)


def running_rows(forget):
    rows = [forget[0:1]]
    for j in range(1, forget.shape[0]):
        rows.append(rows[-1] + forget[j : j + 1])
    return rows


def state_kernel(
    acc_ref, pi_ref, pf_ref, stab_ref, pk_ref, pv_ref, nrm_ref, mem_hbm,
    new_mem_hbm, new_nrm_ref, new_stab_ref, mem_ref, new_mem_ref, ks_ref, vt_ref, decay_ref,
    in_sem, out_sem,
):
    seqs, values, _ = mem_ref.shape
    steps = pi_ref.shape[0]
    rows = seqs * steps
    piece = seqs // STATE_CUTS
    parts = [pl.ds(i * piece, piece) for i in range(STATE_CUTS)]
    loads = [
        pltpu.make_async_copy(mem_hbm.at[p], mem_ref.at[p], in_sem.at[i])
        for i, p in enumerate(parts)
    ]
    stores = [
        pltpu.make_async_copy(new_mem_ref.at[p], new_mem_hbm.at[p], out_sem.at[i])
        for i, p in enumerate(parts)
    ]
    for copy in loads:
        copy.start()
    inflow, forget = kept_gates(pi_ref[...], pf_ref[...], acc_ref[...])
    running = running_rows(forget)
    edge = running[-1]
    stab = stab_ref[...]
    reached = [edge - running[j] + inflow[j : j + 1] for j in range(steps)]
    top = edge + stab
    for r in reached:
        top = jnp.maximum(top, r)
    new_stab_ref[...] = top
    decay = jnp.exp(edge + stab - top)
    row, lane = iota((rows, seqs), 0), iota((rows, seqs), 1)
    picked = jnp.zeros((rows, seqs), F32)
    for j in range(steps):
        picked = jnp.where(row == lane * steps + j, jnp.exp(reached[j] - top), picked)
    share_col = jnp.sum(picked, axis=1, keepdims=True)
    same = iota((seqs, seqs), 0) == iota((seqs, seqs), 1)
    decay_col = jnp.sum(jnp.where(same, decay, 0.0), axis=1, keepdims=True)
    decay_ref[...] = jnp.broadcast_to(decay_col, decay_ref.shape)
    scaled = pk_ref[...].astype(F32) * share_col
    ks_ref[...] = scaled.astype(BF16)
    vt_ref[...] = pv_ref[...].astype(F32).T.astype(BF16)
    member = (iota((seqs, rows), 1) // steps == iota((seqs, rows), 0)).astype(F32).astype(BF16)
    new_nrm_ref[...] = decay_col * nrm_ref[...] + sum(dot(member, p) for p in split(scaled, 3))
    wide = 128 // steps
    group = 4
    owner = iota((values, 128), 1) // steps
    for i in range(STATE_CUTS):
        half = i * piece // wide
        first = i * piece % wide
        ks = ks_ref[half * 128 : (half + 1) * 128, :]
        vt = vt_ref[:, half * 128 : (half + 1) * 128]
        loads[i].wait()
        for g in range(piece // group):
            masks = [
                jnp.where(owner == first + g * group + n, vt, jnp.zeros_like(vt))
                for n in range(group)
            ]
            added = dot(jnp.concatenate(masks, axis=0), ks)
            for n in range(group):
                s = i * piece + g * group + n
                new_mem_ref[s] = (
                    decay_ref[s : s + 1, :] * mem_ref[s]
                    + added[n * values : (n + 1) * values, :]
                )
        stores[i].start()
    for copy in stores:
        copy.wait()


def update_state(accepted, prev_in, prev_forget, stab, pk, pv, normalizer, memory):
    seqs, values, keys = memory.shape
    rows = pk.shape[0]
    vmem = pl.BlockSpec(memory_space=pltpu.VMEM)
    return pl.pallas_call(
        state_kernel,
        name="state",
        out_shape=(
            jax.ShapeDtypeStruct(memory.shape, F32),
            jax.ShapeDtypeStruct(normalizer.shape, F32),
            jax.ShapeDtypeStruct(stab.shape, F32),
        ),
        in_specs=[vmem] * 7 + [pl.BlockSpec(memory_space=pl.ANY)],
        out_specs=(pl.BlockSpec(memory_space=pl.ANY), vmem, vmem),
        scratch_shapes=[
            pltpu.VMEM(memory.shape, F32),
            pltpu.VMEM(memory.shape, F32),
            pltpu.VMEM((rows, keys), BF16),
            pltpu.VMEM((values, rows), BF16),
            pltpu.VMEM((seqs, keys), F32),
            pltpu.SemaphoreType.DMA((STATE_CUTS,)),
            pltpu.SemaphoreType.DMA((STATE_CUTS,)),
        ],
        cost_estimate=pl.CostEstimate(flops=200000000, bytes_accessed=4500000, transcendentals=400),
        compiler_params=pltpu.CompilerParams(vmem_limit_bytes=12 * 1024 * 1024),
    )(accepted, prev_in, prev_forget, stab, pk, pv, normalizer, memory)


def cell_kernel(*refs):
    names = ("xo", "xp", "rest", "gain", "wk", "wv", "wq", "wo", "wi", "wf", "bias", "hg", "acc")
    names += ("pi", "pf", "stab", "pk", "pv", "nrm", "mem", "msg", "nk", "nv", "ni", "nf")
    hbm = dict(zip(names, refs))
    near = list(refs[len(names) :])
    sems = near.pop()
    leaving = []

    def send(src, dst):
        leaving.append(pltpu.make_async_copy(src, dst, sems.at[len(started) + len(leaving)]))
        leaving[-1].start()

    order = ("xo", "xp", "rest", "gain", "w", "wg", "bias", "hg", "acc", "pi", "pf", "stab")
    order += ("pk", "pv", "nrm", "mem", "normed", "mq", "nk", "nv", "ni", "nf")
    at = dict(zip(order, near))
    tp, head = lax.axis_index("tp"), lax.axis_index("kv")
    xo_ref, xp_ref, rest_ref, gain_ref = at["xo"], at["xp"], at["rest"], at["gain"]
    normed_ref, mem_ref, mq_ref = at["normed"], at["mem"], at["mq"]
    blocks, main, lanes = xo_ref.shape
    seqs, values, keys = mem_ref.shape
    steps = at["pi"].shape[0]
    rows = seqs * steps
    heads = at["wg"].shape[0] // 2
    width = gain_ref.shape[1]
    cut = blocks // CUTS
    started = {}

    def bring(key, src, dst):
        started[key] = pltpu.make_async_copy(src, dst, sems.at[len(started)])
        started[key].start()

    bring("rest", hbm["rest"], rest_ref)
    for i in range(CUTS):
        part = pl.ds(i * cut, cut)
        bring(("xo", i), hbm["xo"].at[part], xo_ref.at[part])
        bring(("xp", i), hbm["xp"].at[part], xp_ref.at[part])
    bring("gain", hbm["gain"], gain_ref)
    for i, key in enumerate(("wk", "wv", "wq", "wo")):
        bring(key, hbm[key], at["w"].at[pl.ds(i * keys, keys)])
    for i, key in enumerate(("wi", "wf")):
        bring(key, hbm[key], at["wg"].at[pl.ds(i * heads, heads)])
    small = ("bias", "hg", "acc", "pi", "pf", "stab", "pk", "pv", "nrm")
    for key in (*small, "mem"):
        bring(key, hbm[key], at[key])

    def block(ref, z, side):
        low = rest_ref[2 * z + side]
        return jnp.concatenate([ref[z].astype(F32), low.astype(F32)[: rows - main]], axis=0)

    def square(z, total):
        a, b = block(xo_ref, z, tp), block(xp_ref, z, 1 - tp)
        return total + (a * a + b * b)

    total = jnp.zeros((rows, lanes), F32)
    started["rest"].wait()
    for i in range(CUTS):
        started["xo", i].wait()
        started["xp", i].wait()
        total = lax.fori_loop(i * cut, (i + 1) * cut, square, total, unroll=2)
    inv = lax.rsqrt(jnp.sum(total, axis=1, keepdims=True) / width + EPS)
    inv = jnp.broadcast_to(inv, (rows, lanes))
    started["gain"].wait()

    def normalize(z, carry):
        for ref, side in ((xo_ref, tp), (xp_ref, 1 - tp)):
            to = pl.ds(pl.multiple_of((2 * z + side) * lanes, lanes), lanes)
            normed_ref[:, to] = (block(ref, z, side) * inv * gain_ref[:, to]).astype(BF16)
        return carry

    lax.fori_loop(0, blocks, normalize, 0, unroll=2)
    for key in ("wk", "wv", "wq", "wo", "wi", "wf"):
        started[key].wait()
    normed = normed_ref[...]
    proj = dot_t(normed, at["w"][...])
    gates = dot_t(at["wg"][...], normed)
    for key in small:
        started[key].wait()
    bias_ref, hg_ref, acc_ref, pi_ref, pf_ref = (at[k] for k in ("bias", "hg", "acc", "pi", "pf"))
    stab_ref, pk_ref, pv_ref, nrm_ref = (at[k] for k in ("stab", "pk", "pv", "nrm"))
    nk_ref, nv_ref, ni_ref, nf_ref = (at[k] for k in ("nk", "nv", "ni", "nf"))
    msg_ref = hbm["msg"]

    new_k = proj[:, :keys].astype(BF16)
    new_v = proj[:, keys : keys + values].astype(BF16)
    nk_ref[...] = new_k
    nv_ref[...] = new_v
    send(nk_ref, hbm["nk"])
    send(nv_ref, hbm["nv"])
    query = proj[:, keys + values : 2 * keys + values].astype(BF16)
    out_gate = proj[:, 2 * keys + values :]
    scale = keys ** (-0.5)

    grow = iota(gates.shape, 0)
    gate_in = jnp.sum(jnp.where(grow == head, gates, 0.0), axis=0, keepdims=True)
    gate_forget = jnp.sum(jnp.where(grow == heads + head, gates, 0.0), axis=0, keepdims=True)
    shape = (2 * steps, rows)
    spread = jnp.where(iota(shape, 0) < steps, gate_in, gate_forget)
    spread = jnp.where(iota(shape, 1) % steps == iota(shape, 0) % steps, spread, 0.0)
    member = (iota((rows, seqs), 0) // steps == iota((rows, seqs), 1)).astype(F32).astype(BF16)
    compact = sum(dot(p, member) for p in split(spread, 3))
    bias = bias_ref[...]
    bias = jnp.sum(jnp.where(iota(bias.shape, 1) == head, bias, 0.0), axis=1, keepdims=True)
    new_in = compact[:steps]
    new_forget = log_sigmoid(compact[steps:] + bias)
    ni_ref[...] = new_in
    nf_ref[...] = new_forget
    send(ni_ref, hbm["ni"])
    send(nf_ref, hbm["nf"])
    old_in, old_forget = kept_gates(pi_ref[...], pf_ref[...], acc_ref[...])
    inflow = jnp.concatenate([old_in, new_in], axis=0)
    run = running_rows(jnp.concatenate([old_forget, new_forget], axis=0))
    running = jnp.concatenate(run, axis=0)
    stab = stab_ref[...]
    span = 2 * steps
    place = iota((span, seqs), 0)
    weights, carries, floors = [], [], []
    for t in range(steps):
        latest = run[steps + t]
        d = latest - running + inflow
        d = jnp.where(place <= steps + t, d, FAR_NEGATIVE)
        carried = latest + stab
        top = jnp.maximum(jnp.max(d, axis=0, keepdims=True), carried)
        weights.append(jnp.exp(d - top))
        carries.append(jnp.exp(carried - top))
        floors.append(jnp.exp(-top))

    stacked = jnp.concatenate(weights, axis=0)
    widened = sum(dot_t(p, member) for p in split(stacked, 3))
    keep = iota((span, rows), 0) % steps == iota((span, rows), 1) % steps
    rows_of = [
        jnp.where(keep, widened[t * span : (t + 1) * span], 0.0) for t in range(steps)
    ]
    old_coef = jnp.concatenate(
        [jnp.sum(r[:steps], axis=0, keepdims=True) for r in rows_of], axis=0
    )
    new_coef = jnp.concatenate(
        [jnp.sum(r[steps:], axis=0, keepdims=True) for r in rows_of], axis=0
    )

    def tiled(x, count):
        x = jnp.concatenate([x] * (8 // steps), axis=0)
        return jnp.concatenate([x] * (count // 8), axis=0)

    mine = iota((rows, seqs), 0) // steps == iota((rows, seqs), 1)
    carry_wide = jnp.where(mine, tiled(jnp.concatenate(carries, axis=0), rows), 0.0)
    floor_wide = jnp.where(mine, tiled(jnp.concatenate(floors, axis=0), rows), 0.0)
    carry_scale = jnp.sum(carry_wide, axis=1, keepdims=True)
    least = jnp.sum(floor_wide, axis=1, keepdims=True)
    normal = sum(dot_t(query, p) for p in split(nrm_ref[...], 3))
    carried_normal = jnp.sum(carry_wide * (normal * scale), axis=1, keepdims=True)

    half = rows // 2
    together = iota((half, half), 0) // steps == iota((half, half), 1) // steps
    old_k, old_v = pk_ref[...], pv_ref[...]
    numerators, denominators = [], []
    for h in range(2):
        part = slice(h * half, (h + 1) * half)
        q = query[part]
        numerator = jnp.zeros((half, values), F32)
        denominator = jnp.zeros((half, half), F32)
        for k, v, c in ((old_k, old_v, old_coef), (new_k, new_v, new_coef)):
            score = dot_t(q, k[part]) * scale
            w = jnp.where(together, tiled(c[:, part], half) * score, 0.0)
            denominator = denominator + w
            for p in split(w, 2):
                numerator = numerator + dot(p, v[part])
        numerators.append(numerator)
        denominators.append(jnp.sum(denominator, axis=1, keepdims=True))
    numerator = jnp.concatenate(numerators, axis=0)
    denominator = jnp.concatenate(denominators, axis=0) + carried_normal

    started["mem"].wait()
    group = 4
    span_rows = group * steps
    quarter = iota((span_rows, 2 * values), 0) // steps
    for g in range(seqs // group):
        block_of = mem_ref[g * group : (g + 1) * group].reshape(group * values, keys).astype(BF16)
        full = dot_t(query[g * span_rows : (g + 1) * span_rows, :], block_of)
        side = jnp.where(quarter < 2, full[:, : 2 * values], full[:, 2 * values :])
        mq_ref[g * span_rows : (g + 1) * span_rows, :] = jnp.where(
            quarter[:, :values] % 2 == 0, side[:, :values], side[:, values:]
        )
    numerator = numerator + carry_scale * (mq_ref[...] * scale)
    cell = numerator / jnp.maximum(jnp.abs(denominator), least)
    ones = jnp.ones((8, values), BF16)
    squares = sum(dot_t(ones, p) for p in split(cell * cell, 3))[0:1]
    full_gain = hg_ref[...]
    gain = jnp.sum(jnp.where(iota(full_gain.shape, 0) == head, full_gain, 0.0), axis=0, keepdims=True)
    gain = jnp.where(tp == 0, gain[:, :values], gain[:, values:])
    gated = jax.nn.sigmoid(out_gate) * cell * gain
    msg_ref[:half, :] = jnp.concatenate([gated[:half], gated[half:]], axis=1).astype(BF16)
    high = squares.astype(BF16).astype(F32)
    low = squares - high
    line = iota((PACK, half), 0)
    slab = jnp.where(line == 0, high[:, :half], 0.0)
    slab = jnp.where(line == 1, high[:, half:], slab)
    slab = jnp.where(line == 8, low[:, :half], slab)
    slab = jnp.where(line == 9, low[:, half:], slab)
    msg_ref[half:, :] = slab.astype(BF16)
    for copy in leaving:
        copy.wait()


def run_cell(*args):
    xo, rest, gain, wi = args[0], args[2], args[3], args[8]
    pi, pk, pv, nrm, mem = args[13], *args[16:20]
    rows, keys = pk.shape
    values = pv.shape[1]
    scratch = [pltpu.VMEM(a.shape, a.dtype) for a in (xo, xo, rest, gain)]
    scratch += [
        pltpu.VMEM((2 * keys + 2 * values, gain.shape[1]), BF16),
        pltpu.VMEM((2 * wi.shape[0], gain.shape[1]), BF16),
    ]
    scratch += [pltpu.VMEM(a.shape, a.dtype) for a in args[10:20]]
    scratch += [
        pltpu.VMEM((rows, gain.shape[1]), BF16),
        pltpu.VMEM((rows, values), F32),
        pltpu.VMEM((rows, keys), BF16),
        pltpu.VMEM((rows, values), BF16),
        pltpu.VMEM(pi.shape, F32),
        pltpu.VMEM(pi.shape, F32),
        pltpu.SemaphoreType.DMA((len(args) + 2 * CUTS + 4,)),
    ]
    return pl.pallas_call(
        cell_kernel,
        name="cell",
        out_shape=(
            jax.ShapeDtypeStruct((rows // 2 + PACK, 2 * values), BF16),
            jax.ShapeDtypeStruct((rows, keys), BF16),
            jax.ShapeDtypeStruct((rows, values), BF16),
            jax.ShapeDtypeStruct(pi.shape, F32),
            jax.ShapeDtypeStruct(pi.shape, F32),
        ),
        in_specs=[pl.BlockSpec(memory_space=pl.ANY)] * len(args),
        out_specs=(
            pl.BlockSpec(memory_space=pltpu.VMEM),
            *[pl.BlockSpec(memory_space=pl.ANY)] * 4,
        ),
        scratch_shapes=scratch,
        cost_estimate=pl.CostEstimate(flops=1500000000, bytes_accessed=8000000, transcendentals=100000),
        compiler_params=pltpu.CompilerParams(vmem_limit_bytes=52 * 1024 * 1024),
    )(*args)


def out_kernel(own_ref, other_ref, w_ref, out_ref):
    tp = lax.axis_index("tp")
    heads, tall, _ = own_ref.shape
    half = tall - PACK
    parts, _, chunk, feats = w_ref.shape
    values = parts * chunk
    slab = own_ref[:, half:, :].astype(F32) + other_ref[:, half:, :].astype(F32)
    squares = (slab[:, :8, :] + slab[:, 8:, :]).reshape(heads * 8, half)
    inv = lax.rsqrt(squares / (2 * values) + EPS).T
    zero = jnp.zeros((values, feats), BF16)
    low = jnp.zeros((half, feats), F32)
    high = jnp.zeros((half, feats), F32)
    for h in range(heads):
        sent = jnp.concatenate([own_ref[h, :half, :], other_ref[h, :half, :]], axis=1)
        mine = jnp.concatenate([w_ref[d, 2 * h + tp] for d in range(parts)], axis=0)
        theirs = jnp.concatenate([w_ref[d, 2 * h + 1 - tp] for d in range(parts)], axis=0)
        weight = jnp.concatenate(
            [
                jnp.concatenate([mine, zero, theirs, zero], axis=0),
                jnp.concatenate([zero, mine, zero, theirs], axis=0),
            ],
            axis=1,
        )
        both = dot(sent, weight)
        low = low + inv[:, 8 * h : 8 * h + 1] * both[:, :feats]
        high = high + inv[:, 8 * h + 1 : 8 * h + 2] * both[:, feats:]
    out_ref[:half, :] = low.astype(BF16)
    out_ref[half:, :] = high.astype(BF16)


def project_out(own, other, weight):
    rows = 2 * (own.shape[1] - PACK)
    return pl.pallas_call(
        out_kernel,
        name="mix",
        out_shape=jax.ShapeDtypeStruct((rows, weight.shape[3]), BF16),
        in_specs=[pl.BlockSpec(memory_space=pltpu.VMEM)] * 3,
        cost_estimate=pl.CostEstimate(flops=270000000, bytes_accessed=2000000, transcendentals=10000),
        compiler_params=pltpu.CompilerParams(vmem_limit_bytes=8 * 1024 * 1024),
    )(own, other, weight)


def swap(value, axis):
    size = lax.axis_size(axis)
    return lax.ppermute(value, axis, [(i, size - 1 - i) for i in range(size)])


def shards(
    tokens,
    norm_gain,
    w_query,
    w_key,
    w_value,
    w_outgate,
    w_input,
    w_forget,
    forget_bias,
    head_gain,
    w_out,
    memory,
    normalizer,
    stabilizer,
    prev_keys,
    prev_values,
    prev_input,
    prev_forget,
    accepted,
):
    seqs, steps, lanes = tokens.shape
    rows = seqs * steps
    keys, values = w_query.shape[2], w_value.shape[2]
    kv, tp, dp = lax.axis_size("kv"), lax.axis_size("tp"), lax.axis_size("dp")
    x = tokens.reshape(rows, lanes)
    main = rows - LAST
    chunk = values // dp

    piece = lax.dynamic_slice_in_dim(w_out[0], lax.axis_index("dp") * chunk, chunk, 0)
    piece = piece.reshape(chunk, kv * tp, lanes).transpose(1, 0, 2)
    last = jnp.broadcast_to(x[main:][None], (kv * tp, LAST, lanes))
    packed = jnp.concatenate([last, piece], axis=1)
    first = lax.all_to_all(packed, ("kv", "tp"), 0, 0, tiled=True)
    own = lax.all_gather(x[:main], "kv")
    other = swap(own, "tp")
    piece = first[:, LAST:]
    piece = jnp.broadcast_to(piece[None], (dp, *piece.shape))
    weight = lax.all_to_all(piece, "dp", 0, 0, tiled=True)

    def turned(w):
        return w.transpose(1, 2, 0).reshape(-1, w.shape[0])

    acc = accepted.reshape(1, seqs)
    pi = prev_input.transpose(1, 2, 0).reshape(steps, seqs)
    pf = prev_forget.transpose(1, 2, 0).reshape(steps, seqs)
    stab = stabilizer.transpose(1, 0)
    pk = prev_keys.reshape(rows, keys)
    pv = prev_values.reshape(rows, values)
    nrm = normalizer.reshape(seqs, keys)
    mem = memory.reshape(seqs, values, keys)
    new_memory, new_normalizer, new_stabilizer = update_state(acc, pi, pf, stab, pk, pv, nrm, mem)
    msg, new_keys, new_values, new_input, new_forget = run_cell(
        own, other, first, norm_gain.reshape(1, -1),
        turned(w_key), turned(w_value), turned(w_query), turned(w_outgate), w_input.T, w_forget.T,
        forget_bias.reshape(1, -1), head_gain, acc, pi, pf, stab, pk, pv, nrm, mem,
    )
    gated = lax.all_gather(msg, "kv")
    mixed = project_out(gated, swap(gated, "tp"), weight)
    return (
        mixed.reshape(seqs, steps, lanes),
        new_memory.reshape(memory.shape),
        new_normalizer.reshape(normalizer.shape),
        new_stabilizer.transpose(1, 0),
        new_keys.reshape(prev_keys.shape),
        new_values.reshape(prev_values.shape),
        new_input.reshape(steps, 1, seqs).transpose(2, 0, 1),
        new_forget.reshape(steps, 1, seqs).transpose(2, 0, 1),
    )


def solution(mesh):
    specs = (
        P(("grp", "dp"), None, ("kv", "tp")),
        P(),
        P(None, "kv", None),
        P(None, "kv", None),
        P(None, "kv", "tp"),
        P(None, "kv", "tp"),
        P(),
        P(),
        P(),
        P(),
        P("kv", "tp", None),
        P(("grp", "dp"), "kv", "tp", None),
        P(("grp", "dp"), "kv", None),
        P(("grp", "dp"), "kv"),
        P(("grp", "dp"), None, "kv", None),
        P(("grp", "dp"), None, "kv", "tp"),
        P(("grp", "dp"), None, "kv"),
        P(("grp", "dp"), None, "kv"),
        P(("grp", "dp")),
    )
    outs = (
        P(("grp", "dp"), None, ("kv", "tp")),
        P(("grp", "dp"), "kv", "tp", None),
        P(("grp", "dp"), "kv", None),
        P(("grp", "dp"), "kv"),
        P(("grp", "dp"), None, "kv", None),
        P(("grp", "dp"), None, "kv", "tp"),
        P(("grp", "dp"), None, "kv"),
        P(("grp", "dp"), None, "kv"),
    )

    return jax.shard_map(shards, mesh=mesh, in_specs=specs, out_specs=outs, check_vma=False)
```

```python
import jax
import jax.numpy as jnp
from jax import lax
from jax.experimental import pallas as pl
from jax.experimental.pallas import tpu as pltpu
from jax.sharding import PartitionSpec as P


EPS = 1e-06
FAR_NEGATIVE = -1e30
F32 = jnp.float32
BF16 = jnp.bfloat16
STATE_CUTS = 4
CUTS = 4
SHARE = 4
LAST = 8
PACK = 16


def iota(shape, dim):
    return lax.broadcasted_iota(jnp.int32, shape, dim)


def dot(a, b, precision=None):
    return jnp.dot(a, b, preferred_element_type=F32, precision=precision)


def dot_t(a, b, precision=None):
    return lax.dot_general(
        a, b, (((1,), (1,)), ((), ())), preferred_element_type=F32, precision=precision
    )


def split(x, parts):
    pieces = []
    for _ in range(parts):
        piece = x.astype(BF16)
        pieces.append(piece)
        x = x - piece.astype(F32)
    return pieces


def log_sigmoid(x):
    return jnp.minimum(x, 0.0) - jnp.log1p(jnp.exp(-jnp.abs(x)))


def kept_gates(prev_in, prev_forget, accepted):
    dropped = iota(prev_in.shape, 0) >= accepted
    return jnp.where(dropped, FAR_NEGATIVE, prev_in), jnp.where(dropped, 0.0, prev_forget)


def running_rows(forget):
    rows = [forget[0:1]]
    for j in range(1, forget.shape[0]):
        rows.append(rows[-1] + forget[j : j + 1])
    return rows


def state_kernel(
    acc_ref, pi_ref, pf_ref, stab_ref, pk_ref, pv_ref, nrm_ref, mem_hbm,
    new_mem_hbm, new_nrm_ref, new_stab_ref, mem_ref, new_mem_ref, ks_ref, vt_ref, decay_ref,
    in_sem, out_sem,
):
    seqs, values, _ = mem_ref.shape
    steps = pi_ref.shape[0]
    rows = seqs * steps
    piece = seqs // STATE_CUTS
    parts = [pl.ds(i * piece, piece) for i in range(STATE_CUTS)]
    loads = [
        pltpu.make_async_copy(mem_hbm.at[p], mem_ref.at[p], in_sem.at[i])
        for i, p in enumerate(parts)
    ]
    stores = [
        pltpu.make_async_copy(new_mem_ref.at[p], new_mem_hbm.at[p], out_sem.at[i])
        for i, p in enumerate(parts)
    ]
    for copy in loads:
        copy.start()
    inflow, forget = kept_gates(pi_ref[...], pf_ref[...], acc_ref[...])
    running = running_rows(forget)
    edge = running[-1]
    stab = stab_ref[...]
    reached = [edge - running[j] + inflow[j : j + 1] for j in range(steps)]
    top = edge + stab
    for r in reached:
        top = jnp.maximum(top, r)
    new_stab_ref[...] = top
    decay = jnp.exp(edge + stab - top)
    row, lane = iota((rows, seqs), 0), iota((rows, seqs), 1)
    picked = jnp.zeros((rows, seqs), F32)
    for j in range(steps):
        picked = jnp.where(row == lane * steps + j, jnp.exp(reached[j] - top), picked)
    share_col = jnp.sum(picked, axis=1, keepdims=True)
    same = iota((seqs, seqs), 0) == iota((seqs, seqs), 1)
    decay_col = jnp.sum(jnp.where(same, decay, 0.0), axis=1, keepdims=True)
    decay_ref[...] = jnp.broadcast_to(decay_col, decay_ref.shape)
    scaled = pk_ref[...].astype(F32) * share_col
    ks_ref[...] = scaled.astype(BF16)
    vt_ref[...] = pv_ref[...].astype(F32).T.astype(BF16)
    member = (iota((seqs, rows), 1) // steps == iota((seqs, rows), 0)).astype(F32).astype(BF16)
    new_nrm_ref[...] = decay_col * nrm_ref[...] + sum(dot(member, p) for p in split(scaled, 3))
    wide = 128 // steps
    group = 4
    owner = iota((values, 128), 1) // steps
    for i in range(STATE_CUTS):
        half = i * piece // wide
        first = i * piece % wide
        ks = ks_ref[half * 128 : (half + 1) * 128, :]
        vt = vt_ref[:, half * 128 : (half + 1) * 128]
        loads[i].wait()
        for g in range(piece // group):
            masks = [
                jnp.where(owner == first + g * group + n, vt, jnp.zeros_like(vt))
                for n in range(group)
            ]
            added = dot(jnp.concatenate(masks, axis=0), ks)
            for n in range(group):
                s = i * piece + g * group + n
                new_mem_ref[s] = (
                    decay_ref[s : s + 1, :] * mem_ref[s]
                    + added[n * values : (n + 1) * values, :]
                )
        stores[i].start()
    for copy in stores:
        copy.wait()


def update_state(accepted, prev_in, prev_forget, stab, pk, pv, normalizer, memory):
    seqs, values, keys = memory.shape
    rows = pk.shape[0]
    vmem = pl.BlockSpec(memory_space=pltpu.VMEM)
    return pl.pallas_call(
        state_kernel,
        name="state",
        out_shape=(
            jax.ShapeDtypeStruct(memory.shape, F32),
            jax.ShapeDtypeStruct(normalizer.shape, F32),
            jax.ShapeDtypeStruct(stab.shape, F32),
        ),
        in_specs=[vmem] * 7 + [pl.BlockSpec(memory_space=pl.ANY)],
        out_specs=(pl.BlockSpec(memory_space=pl.ANY), vmem, vmem),
        scratch_shapes=[
            pltpu.VMEM(memory.shape, F32),
            pltpu.VMEM(memory.shape, F32),
            pltpu.VMEM((rows, keys), BF16),
            pltpu.VMEM((values, rows), BF16),
            pltpu.VMEM((seqs, keys), F32),
            pltpu.SemaphoreType.DMA((STATE_CUTS,)),
            pltpu.SemaphoreType.DMA((STATE_CUTS,)),
        ],
        cost_estimate=pl.CostEstimate(flops=200000000, bytes_accessed=4500000, transcendentals=400),
        compiler_params=pltpu.CompilerParams(vmem_limit_bytes=12 * 1024 * 1024),
    )(accepted, prev_in, prev_forget, stab, pk, pv, normalizer, memory)


def cell_kernel(*refs):
    names = ("xo", "xp", "rest", "gain", "wk", "wv", "wq", "wo", "wi", "wf", "bias", "hg", "acc")
    names += ("pi", "pf", "stab", "pk", "pv", "nrm", "mem", "msg", "nk", "nv", "ni", "nf")
    hbm = dict(zip(names, refs))
    near = list(refs[len(names) :])
    sems = near.pop()
    leaving = []

    def send(src, dst):
        leaving.append(pltpu.make_async_copy(src, dst, sems.at[len(started) + len(leaving)]))
        leaving[-1].start()

    order = ("xo", "xp", "rest", "gain", "w", "wg", "bias", "hg", "acc", "pi", "pf", "stab")
    order += ("pk", "pv", "nrm", "mem", "normed", "mq", "nk", "nv", "ni", "nf")
    at = dict(zip(order, near))
    tp, head = lax.axis_index("tp"), lax.axis_index("kv")
    xo_ref, xp_ref, rest_ref, gain_ref = at["xo"], at["xp"], at["rest"], at["gain"]
    normed_ref, mem_ref, mq_ref = at["normed"], at["mem"], at["mq"]
    blocks, main, lanes = xo_ref.shape
    seqs, values, keys = mem_ref.shape
    steps = at["pi"].shape[0]
    rows = seqs * steps
    heads = at["wg"].shape[0] // 2
    width = gain_ref.shape[1]
    cut = blocks // CUTS
    started = {}

    def bring(key, src, dst):
        started[key] = pltpu.make_async_copy(src, dst, sems.at[len(started)])
        started[key].start()

    bring("rest", hbm["rest"], rest_ref)
    for i in range(CUTS):
        part = pl.ds(i * cut, cut)
        bring(("xo", i), hbm["xo"].at[part], xo_ref.at[part])
        bring(("xp", i), hbm["xp"].at[part], xp_ref.at[part])
    bring("gain", hbm["gain"], gain_ref)
    for i, key in enumerate(("wk", "wv", "wq", "wo")):
        bring(key, hbm[key], at["w"].at[pl.ds(i * keys, keys)])
    for i, key in enumerate(("wi", "wf")):
        bring(key, hbm[key], at["wg"].at[pl.ds(i * heads, heads)])
    small = ("bias", "hg", "acc", "pi", "pf", "stab", "pk", "pv", "nrm")
    for key in (*small, "mem"):
        bring(key, hbm[key], at[key])

    def block(ref, z, side):
        low = rest_ref[2 * z + side]
        return jnp.concatenate([ref[z].astype(F32), low.astype(F32)[: rows - main]], axis=0)

    def square(z, total):
        a, b = block(xo_ref, z, tp), block(xp_ref, z, 1 - tp)
        return total + (a * a + b * b)

    total = jnp.zeros((rows, lanes), F32)
    started["rest"].wait()
    for i in range(CUTS):
        started["xo", i].wait()
        started["xp", i].wait()
        total = lax.fori_loop(i * cut, (i + 1) * cut, square, total, unroll=2)
    inv = lax.rsqrt(jnp.sum(total, axis=1, keepdims=True) / width + EPS)
    inv = jnp.broadcast_to(inv, (rows, lanes))
    started["gain"].wait()

    def normalize(z, carry):
        for ref, side in ((xo_ref, tp), (xp_ref, 1 - tp)):
            to = pl.ds(pl.multiple_of((2 * z + side) * lanes, lanes), lanes)
            normed_ref[:, to] = (block(ref, z, side) * inv * gain_ref[:, to]).astype(BF16)
        return carry

    lax.fori_loop(0, blocks, normalize, 0, unroll=2)
    for key in ("wk", "wv", "wq", "wo", "wi", "wf"):
        started[key].wait()
    normed = normed_ref[...]
    proj = dot_t(normed, at["w"][...])
    gates = dot_t(at["wg"][...], normed)
    for key in small:
        started[key].wait()
    bias_ref, hg_ref, acc_ref, pi_ref, pf_ref = (at[k] for k in ("bias", "hg", "acc", "pi", "pf"))
    stab_ref, pk_ref, pv_ref, nrm_ref = (at[k] for k in ("stab", "pk", "pv", "nrm"))
    nk_ref, nv_ref, ni_ref, nf_ref = (at[k] for k in ("nk", "nv", "ni", "nf"))
    msg_ref = hbm["msg"]

    new_k = proj[:, :keys].astype(BF16)
    new_v = proj[:, keys : keys + values].astype(BF16)
    nk_ref[...] = new_k
    nv_ref[...] = new_v
    send(nk_ref, hbm["nk"])
    send(nv_ref, hbm["nv"])
    query = proj[:, keys + values : 2 * keys + values].astype(BF16)
    out_gate = proj[:, 2 * keys + values :]
    scale = keys ** (-0.5)

    grow = iota(gates.shape, 0)
    gate_in = jnp.sum(jnp.where(grow == head, gates, 0.0), axis=0, keepdims=True)
    gate_forget = jnp.sum(jnp.where(grow == heads + head, gates, 0.0), axis=0, keepdims=True)
    shape = (2 * steps, rows)
    spread = jnp.where(iota(shape, 0) < steps, gate_in, gate_forget)
    spread = jnp.where(iota(shape, 1) % steps == iota(shape, 0) % steps, spread, 0.0)
    member = (iota((rows, seqs), 0) // steps == iota((rows, seqs), 1)).astype(F32).astype(BF16)
    compact = sum(dot(p, member) for p in split(spread, 3))
    bias = bias_ref[...]
    bias = jnp.sum(jnp.where(iota(bias.shape, 1) == head, bias, 0.0), axis=1, keepdims=True)
    new_in = compact[:steps]
    new_forget = log_sigmoid(compact[steps:] + bias)
    ni_ref[...] = new_in
    nf_ref[...] = new_forget
    send(ni_ref, hbm["ni"])
    send(nf_ref, hbm["nf"])
    old_in, old_forget = kept_gates(pi_ref[...], pf_ref[...], acc_ref[...])
    inflow = jnp.concatenate([old_in, new_in], axis=0)
    run = running_rows(jnp.concatenate([old_forget, new_forget], axis=0))
    running = jnp.concatenate(run, axis=0)
    stab = stab_ref[...]
    span = 2 * steps
    place = iota((span, seqs), 0)
    weights, carries, floors = [], [], []
    for t in range(steps):
        latest = run[steps + t]
        d = latest - running + inflow
        d = jnp.where(place <= steps + t, d, FAR_NEGATIVE)
        carried = latest + stab
        top = jnp.maximum(jnp.max(d, axis=0, keepdims=True), carried)
        weights.append(jnp.exp(d - top))
        carries.append(jnp.exp(carried - top))
        floors.append(jnp.exp(-top))

    stacked = jnp.concatenate(weights, axis=0)
    widened = sum(dot_t(p, member) for p in split(stacked, 3))
    keep = iota((span, rows), 0) % steps == iota((span, rows), 1) % steps
    rows_of = [
        jnp.where(keep, widened[t * span : (t + 1) * span], 0.0) for t in range(steps)
    ]
    old_coef = jnp.concatenate(
        [jnp.sum(r[:steps], axis=0, keepdims=True) for r in rows_of], axis=0
    )
    new_coef = jnp.concatenate(
        [jnp.sum(r[steps:], axis=0, keepdims=True) for r in rows_of], axis=0
    )

    def tiled(x, count):
        x = jnp.concatenate([x] * (8 // steps), axis=0)
        return jnp.concatenate([x] * (count // 8), axis=0)

    mine = iota((rows, seqs), 0) // steps == iota((rows, seqs), 1)
    carry_wide = jnp.where(mine, tiled(jnp.concatenate(carries, axis=0), rows), 0.0)
    floor_wide = jnp.where(mine, tiled(jnp.concatenate(floors, axis=0), rows), 0.0)
    carry_scale = jnp.sum(carry_wide, axis=1, keepdims=True)
    least = jnp.sum(floor_wide, axis=1, keepdims=True)
    normal = sum(dot_t(query, p) for p in split(nrm_ref[...], 3))
    carried_normal = jnp.sum(carry_wide * (normal * scale), axis=1, keepdims=True)

    half = rows // 2
    together = iota((half, half), 0) // steps == iota((half, half), 1) // steps
    old_k, old_v = pk_ref[...], pv_ref[...]
    numerators, denominators = [], []
    for h in range(2):
        part = slice(h * half, (h + 1) * half)
        q = query[part]
        numerator = jnp.zeros((half, values), F32)
        denominator = jnp.zeros((half, half), F32)
        for k, v, c in ((old_k, old_v, old_coef), (new_k, new_v, new_coef)):
            score = dot_t(q, k[part]) * scale
            w = jnp.where(together, tiled(c[:, part], half) * score, 0.0)
            denominator = denominator + w
            for p in split(w, 2):
                numerator = numerator + dot(p, v[part])
        numerators.append(numerator)
        denominators.append(jnp.sum(denominator, axis=1, keepdims=True))
    numerator = jnp.concatenate(numerators, axis=0)
    denominator = jnp.concatenate(denominators, axis=0) + carried_normal

    started["mem"].wait()
    group = 4
    span_rows = group * steps
    quarter = iota((span_rows, 2 * values), 0) // steps
    for g in range(seqs // group):
        block_of = mem_ref[g * group : (g + 1) * group].reshape(group * values, keys).astype(BF16)
        full = dot_t(query[g * span_rows : (g + 1) * span_rows, :], block_of)
        side = jnp.where(quarter < 2, full[:, : 2 * values], full[:, 2 * values :])
        mq_ref[g * span_rows : (g + 1) * span_rows, :] = jnp.where(
            quarter[:, :values] % 2 == 0, side[:, :values], side[:, values:]
        )
    numerator = numerator + carry_scale * (mq_ref[...] * scale)
    cell = numerator / jnp.maximum(jnp.abs(denominator), least)
    ones = jnp.ones((8, values), BF16)
    squares = sum(dot_t(ones, p) for p in split(cell * cell, 3))[0:1]
    full_gain = hg_ref[...]
    gain = jnp.sum(jnp.where(iota(full_gain.shape, 0) == head, full_gain, 0.0), axis=0, keepdims=True)
    gain = jnp.where(tp == 0, gain[:, :values], gain[:, values:])
    gated = jax.nn.sigmoid(out_gate) * cell * gain
    msg_ref[:half, :] = jnp.concatenate([gated[:half], gated[half:]], axis=1).astype(BF16)
    high = squares.astype(BF16).astype(F32)
    low = squares - high
    line = iota((PACK, half), 0)
    slab = jnp.where(line == 0, high[:, :half], 0.0)
    slab = jnp.where(line == 1, high[:, half:], slab)
    slab = jnp.where(line == 8, low[:, :half], slab)
    slab = jnp.where(line == 9, low[:, half:], slab)
    msg_ref[half:, :] = slab.astype(BF16)
    for copy in leaving:
        copy.wait()


def run_cell(*args):
    xo, rest, gain, wi = args[0], args[2], args[3], args[8]
    pi, pk, pv, nrm, mem = args[13], *args[16:20]
    rows, keys = pk.shape
    values = pv.shape[1]
    scratch = [pltpu.VMEM(a.shape, a.dtype) for a in (xo, xo, rest, gain)]
    scratch += [
        pltpu.VMEM((2 * keys + 2 * values, gain.shape[1]), BF16),
        pltpu.VMEM((2 * wi.shape[0], gain.shape[1]), BF16),
    ]
    scratch += [pltpu.VMEM(a.shape, a.dtype) for a in args[10:20]]
    scratch += [
        pltpu.VMEM((rows, gain.shape[1]), BF16),
        pltpu.VMEM((rows, values), F32),
        pltpu.VMEM((rows, keys), BF16),
        pltpu.VMEM((rows, values), BF16),
        pltpu.VMEM(pi.shape, F32),
        pltpu.VMEM(pi.shape, F32),
        pltpu.SemaphoreType.DMA((len(args) + 2 * CUTS + 4,)),
    ]
    return pl.pallas_call(
        cell_kernel,
        name="cell",
        out_shape=(
            jax.ShapeDtypeStruct((rows // 2 + PACK, 2 * values), BF16),
            jax.ShapeDtypeStruct((rows, keys), BF16),
            jax.ShapeDtypeStruct((rows, values), BF16),
            jax.ShapeDtypeStruct(pi.shape, F32),
            jax.ShapeDtypeStruct(pi.shape, F32),
        ),
        in_specs=[pl.BlockSpec(memory_space=pl.ANY)] * len(args),
        out_specs=(
            pl.BlockSpec(memory_space=pltpu.VMEM),
            *[pl.BlockSpec(memory_space=pl.ANY)] * 4,
        ),
        scratch_shapes=scratch,
        cost_estimate=pl.CostEstimate(flops=1500000000, bytes_accessed=8000000, transcendentals=100000),
        compiler_params=pltpu.CompilerParams(vmem_limit_bytes=56 * 1024 * 1024),
    )(*args)


def out_kernel(own_ref, other_ref, w_ref, out_ref):
    tp = lax.axis_index("tp")
    heads, tall, _ = own_ref.shape
    half = tall - PACK
    parts, _, chunk, feats = w_ref.shape
    values = parts * chunk
    slab = own_ref[:, half:, :].astype(F32) + other_ref[:, half:, :].astype(F32)
    squares = (slab[:, :8, :] + slab[:, 8:, :]).reshape(heads * 8, half)
    inv = lax.rsqrt(squares / (2 * values) + EPS).T
    zero = jnp.zeros((values, feats), BF16)
    low = jnp.zeros((half, feats), F32)
    high = jnp.zeros((half, feats), F32)
    for h in range(heads):
        sent = jnp.concatenate([own_ref[h, :half, :], other_ref[h, :half, :]], axis=1)
        mine = jnp.concatenate([w_ref[d, 2 * h + tp] for d in range(parts)], axis=0)
        theirs = jnp.concatenate([w_ref[d, 2 * h + 1 - tp] for d in range(parts)], axis=0)
        weight = jnp.concatenate(
            [
                jnp.concatenate([mine, zero, theirs, zero], axis=0),
                jnp.concatenate([zero, mine, zero, theirs], axis=0),
            ],
            axis=1,
        )
        both = dot(sent, weight)
        low = low + inv[:, 8 * h : 8 * h + 1] * both[:, :feats]
        high = high + inv[:, 8 * h + 1 : 8 * h + 2] * both[:, feats:]
    out_ref[:half, :] = low.astype(BF16)
    out_ref[half:, :] = high.astype(BF16)


def project_out(own, other, weight):
    rows = 2 * (own.shape[1] - PACK)
    return pl.pallas_call(
        out_kernel,
        name="mix",
        out_shape=jax.ShapeDtypeStruct((rows, weight.shape[3]), BF16),
        in_specs=[pl.BlockSpec(memory_space=pltpu.VMEM)] * 3,
        cost_estimate=pl.CostEstimate(flops=270000000, bytes_accessed=2000000, transcendentals=10000),
        compiler_params=pltpu.CompilerParams(vmem_limit_bytes=8 * 1024 * 1024),
    )(own, other, weight)


def swap(value, axis):
    size = lax.axis_size(axis)
    return lax.ppermute(value, axis, [(i, size - 1 - i) for i in range(size)])


def shards(
    tokens,
    norm_gain,
    w_query,
    w_key,
    w_value,
    w_outgate,
    w_input,
    w_forget,
    forget_bias,
    head_gain,
    w_out,
    memory,
    normalizer,
    stabilizer,
    prev_keys,
    prev_values,
    prev_input,
    prev_forget,
    accepted,
):
    seqs, steps, lanes = tokens.shape
    rows = seqs * steps
    keys, values = w_query.shape[2], w_value.shape[2]
    kv, tp, dp = lax.axis_size("kv"), lax.axis_size("tp"), lax.axis_size("dp")
    x = tokens.reshape(rows, lanes)
    main = rows - LAST
    share = min(dp, SHARE)
    chunk = values // share

    piece = lax.dynamic_slice_in_dim(w_out[0], lax.axis_index("dp") % share * chunk, chunk, 0)
    piece = piece.reshape(chunk, kv * tp, lanes).transpose(1, 0, 2)
    last = jnp.broadcast_to(x[main:][None], (kv * tp, LAST, lanes))
    packed = jnp.concatenate([last, piece], axis=1)
    first = lax.all_to_all(packed, ("kv", "tp"), 0, 0, tiled=True)
    own = lax.all_gather(x[:main], "kv")
    other = swap(own, "tp")
    piece = first[:, LAST:]
    piece = jnp.broadcast_to(piece[None], (share, *piece.shape))
    groups = [list(range(i, i + share)) for i in range(0, dp, share)]
    weight = lax.all_to_all(piece, "dp", 0, 0, tiled=True, axis_index_groups=groups)

    def turned(w):
        return w.transpose(1, 2, 0).reshape(-1, w.shape[0])

    acc = accepted.reshape(1, seqs)
    pi = prev_input.transpose(1, 2, 0).reshape(steps, seqs)
    pf = prev_forget.transpose(1, 2, 0).reshape(steps, seqs)
    stab = stabilizer.transpose(1, 0)
    pk = prev_keys.reshape(rows, keys)
    pv = prev_values.reshape(rows, values)
    nrm = normalizer.reshape(seqs, keys)
    mem = memory.reshape(seqs, values, keys)
    new_memory, new_normalizer, new_stabilizer = update_state(acc, pi, pf, stab, pk, pv, nrm, mem)
    msg, new_keys, new_values, new_input, new_forget = run_cell(
        own, other, first, norm_gain.reshape(1, -1),
        turned(w_key), turned(w_value), turned(w_query), turned(w_outgate), w_input.T, w_forget.T,
        forget_bias.reshape(1, -1), head_gain, acc, pi, pf, stab, pk, pv, nrm, mem,
    )
    gated = lax.all_gather(msg, "kv")
    mixed = project_out(gated, swap(gated, "tp"), weight)
    return (
        mixed.reshape(seqs, steps, lanes),
        new_memory.reshape(memory.shape),
        new_normalizer.reshape(normalizer.shape),
        new_stabilizer.transpose(1, 0),
        new_keys.reshape(prev_keys.shape),
        new_values.reshape(prev_values.shape),
        new_input.reshape(steps, 1, seqs).transpose(2, 0, 1),
        new_forget.reshape(steps, 1, seqs).transpose(2, 0, 1),
    )


def solution(mesh):
    specs = (
        P(("grp", "dp"), None, ("kv", "tp")),
        P(),
        P(None, "kv", None),
        P(None, "kv", None),
        P(None, "kv", "tp"),
        P(None, "kv", "tp"),
        P(),
        P(),
        P(),
        P(),
        P("kv", "tp", None),
        P(("grp", "dp"), "kv", "tp", None),
        P(("grp", "dp"), "kv", None),
        P(("grp", "dp"), "kv"),
        P(("grp", "dp"), None, "kv", None),
        P(("grp", "dp"), None, "kv", "tp"),
        P(("grp", "dp"), None, "kv"),
        P(("grp", "dp"), None, "kv"),
        P(("grp", "dp")),
    )
    outs = (
        P(("grp", "dp"), None, ("kv", "tp")),
        P(("grp", "dp"), "kv", "tp", None),
        P(("grp", "dp"), "kv", None),
        P(("grp", "dp"), "kv"),
        P(("grp", "dp"), None, "kv", None),
        P(("grp", "dp"), None, "kv", "tp"),
        P(("grp", "dp"), None, "kv"),
        P(("grp", "dp"), None, "kv"),
    )

    return jax.shard_map(shards, mesh=mesh, in_specs=specs, out_specs=outs, check_vma=False)
```

```python
import jax
import jax.numpy as jnp
from jax import lax
from jax.experimental import pallas as pl
from jax.experimental.pallas import tpu as pltpu
from jax.sharding import PartitionSpec as P


EPS = 1e-06
FAR_NEGATIVE = -1e30
F32 = jnp.float32
BF16 = jnp.bfloat16
STATE_CUTS = 8
CUTS = 4
SHARE = 8
LAST = 8
PACK = 16


def iota(shape, dim):
    return lax.broadcasted_iota(jnp.int32, shape, dim)


def dot(a, b, precision=None):
    return jnp.dot(a, b, preferred_element_type=F32, precision=precision)


def dot_t(a, b, precision=None):
    return lax.dot_general(
        a, b, (((1,), (1,)), ((), ())), preferred_element_type=F32, precision=precision
    )


def split(x, parts):
    pieces = []
    for _ in range(parts):
        piece = x.astype(BF16)
        pieces.append(piece)
        x = x - piece.astype(F32)
    return pieces


def log_sigmoid(x):
    return jnp.minimum(x, 0.0) - jnp.log1p(jnp.exp(-jnp.abs(x)))


def kept_gates(prev_in, prev_forget, accepted):
    dropped = iota(prev_in.shape, 0) >= accepted
    return jnp.where(dropped, FAR_NEGATIVE, prev_in), jnp.where(dropped, 0.0, prev_forget)


def running_rows(forget):
    rows = [forget[0:1]]
    for j in range(1, forget.shape[0]):
        rows.append(rows[-1] + forget[j : j + 1])
    return rows


def state_kernel(
    acc_ref, pi_ref, pf_ref, stab_ref, pk_ref, pv_ref, nrm_ref, mem_hbm,
    new_mem_hbm, new_nrm_ref, new_stab_ref, mem_ref, new_mem_ref, ks_ref, vt_ref, decay_ref,
    in_sem, out_sem,
):
    seqs, values, _ = mem_ref.shape
    steps = pi_ref.shape[0]
    rows = seqs * steps
    piece = seqs // STATE_CUTS
    parts = [pl.ds(i * piece, piece) for i in range(STATE_CUTS)]
    loads = [
        pltpu.make_async_copy(mem_hbm.at[p], mem_ref.at[p], in_sem.at[i])
        for i, p in enumerate(parts)
    ]
    stores = [
        pltpu.make_async_copy(new_mem_ref.at[p], new_mem_hbm.at[p], out_sem.at[i])
        for i, p in enumerate(parts)
    ]
    for copy in loads:
        copy.start()
    inflow, forget = kept_gates(pi_ref[...], pf_ref[...], acc_ref[...])
    running = running_rows(forget)
    edge = running[-1]
    stab = stab_ref[...]
    reached = [edge - running[j] + inflow[j : j + 1] for j in range(steps)]
    top = edge + stab
    for r in reached:
        top = jnp.maximum(top, r)
    new_stab_ref[...] = top
    decay = jnp.exp(edge + stab - top)
    row, lane = iota((rows, seqs), 0), iota((rows, seqs), 1)
    picked = jnp.zeros((rows, seqs), F32)
    for j in range(steps):
        picked = jnp.where(row == lane * steps + j, jnp.exp(reached[j] - top), picked)
    share_col = jnp.sum(picked, axis=1, keepdims=True)
    same = iota((seqs, seqs), 0) == iota((seqs, seqs), 1)
    decay_col = jnp.sum(jnp.where(same, decay, 0.0), axis=1, keepdims=True)
    decay_ref[...] = jnp.broadcast_to(decay_col, decay_ref.shape)
    scaled = pk_ref[...].astype(F32) * share_col
    ks_ref[...] = scaled.astype(BF16)
    vt_ref[...] = pv_ref[...].astype(F32).T.astype(BF16)
    member = (iota((seqs, rows), 1) // steps == iota((seqs, rows), 0)).astype(F32).astype(BF16)
    new_nrm_ref[...] = decay_col * nrm_ref[...] + sum(dot(member, p) for p in split(scaled, 3))
    wide = 128 // steps
    group = 4
    owner = iota((values, 128), 1) // steps
    for i in range(STATE_CUTS):
        half = i * piece // wide
        first = i * piece % wide
        ks = ks_ref[half * 128 : (half + 1) * 128, :]
        vt = vt_ref[:, half * 128 : (half + 1) * 128]
        loads[i].wait()
        for g in range(piece // group):
            masks = [
                jnp.where(owner == first + g * group + n, vt, jnp.zeros_like(vt))
                for n in range(group)
            ]
            added = dot(jnp.concatenate(masks, axis=0), ks)
            for n in range(group):
                s = i * piece + g * group + n
                new_mem_ref[s] = (
                    decay_ref[s : s + 1, :] * mem_ref[s]
                    + added[n * values : (n + 1) * values, :]
                )
        stores[i].start()
    for copy in stores:
        copy.wait()


def update_state(accepted, prev_in, prev_forget, stab, pk, pv, normalizer, memory):
    seqs, values, keys = memory.shape
    rows = pk.shape[0]
    vmem = pl.BlockSpec(memory_space=pltpu.VMEM)
    return pl.pallas_call(
        state_kernel,
        name="state",
        out_shape=(
            jax.ShapeDtypeStruct(memory.shape, F32),
            jax.ShapeDtypeStruct(normalizer.shape, F32),
            jax.ShapeDtypeStruct(stab.shape, F32),
        ),
        in_specs=[vmem] * 7 + [pl.BlockSpec(memory_space=pl.ANY)],
        out_specs=(pl.BlockSpec(memory_space=pl.ANY), vmem, vmem),
        scratch_shapes=[
            pltpu.VMEM(memory.shape, F32),
            pltpu.VMEM(memory.shape, F32),
            pltpu.VMEM((rows, keys), BF16),
            pltpu.VMEM((values, rows), BF16),
            pltpu.VMEM((seqs, keys), F32),
            pltpu.SemaphoreType.DMA((STATE_CUTS,)),
            pltpu.SemaphoreType.DMA((STATE_CUTS,)),
        ],
        cost_estimate=pl.CostEstimate(flops=200000000, bytes_accessed=4500000, transcendentals=400),
        compiler_params=pltpu.CompilerParams(vmem_limit_bytes=12 * 1024 * 1024),
    )(accepted, prev_in, prev_forget, stab, pk, pv, normalizer, memory)


def cell_kernel(*refs):
    names = ("xo", "xp", "rest", "gain", "wk", "wv", "wq", "wo", "wi", "wf", "bias", "hg", "acc")
    names += ("pi", "pf", "stab", "pk", "pv", "nrm", "mem", "msg", "nk", "nv", "ni", "nf")
    hbm = dict(zip(names, refs))
    near = list(refs[len(names) :])
    sems = near.pop()
    leaving = []

    def send(src, dst):
        leaving.append(pltpu.make_async_copy(src, dst, sems.at[len(started) + len(leaving)]))
        leaving[-1].start()

    order = ("xo", "xp", "rest", "gain", "w", "wg", "bias", "hg", "acc", "pi", "pf", "stab")
    order += ("pk", "pv", "nrm", "mem", "normed", "mq", "nk", "nv", "ni", "nf")
    at = dict(zip(order, near))
    tp, head = lax.axis_index("tp"), lax.axis_index("kv")
    xo_ref, xp_ref, rest_ref, gain_ref = at["xo"], at["xp"], at["rest"], at["gain"]
    normed_ref, mem_ref, mq_ref = at["normed"], at["mem"], at["mq"]
    blocks, main, lanes = xo_ref.shape
    seqs, values, keys = mem_ref.shape
    steps = at["pi"].shape[0]
    rows = seqs * steps
    heads = at["wg"].shape[0] // 2
    width = gain_ref.shape[1]
    cut = blocks // CUTS
    started = {}

    def bring(key, src, dst):
        started[key] = pltpu.make_async_copy(src, dst, sems.at[len(started)])
        started[key].start()

    bring("rest", hbm["rest"], rest_ref)
    for i in range(CUTS):
        part = pl.ds(i * cut, cut)
        bring(("xo", i), hbm["xo"].at[part], xo_ref.at[part])
        bring(("xp", i), hbm["xp"].at[part], xp_ref.at[part])
    bring("gain", hbm["gain"], gain_ref)
    for i, key in enumerate(("wk", "wv", "wq", "wo")):
        bring(key, hbm[key], at["w"].at[pl.ds(i * keys, keys)])
    for i, key in enumerate(("wi", "wf")):
        bring(key, hbm[key], at["wg"].at[pl.ds(i * heads, heads)])
    small = ("bias", "hg", "acc", "pi", "pf", "stab", "pk", "pv", "nrm")
    for key in (*small, "mem"):
        bring(key, hbm[key], at[key])

    def block(ref, z, side):
        low = rest_ref[2 * z + side]
        return jnp.concatenate([ref[z].astype(F32), low.astype(F32)[: rows - main]], axis=0)

    def square(z, total):
        a, b = block(xo_ref, z, tp), block(xp_ref, z, 1 - tp)
        return total + (a * a + b * b)

    total = jnp.zeros((rows, lanes), F32)
    started["rest"].wait()
    for i in range(CUTS):
        started["xo", i].wait()
        started["xp", i].wait()
        total = lax.fori_loop(i * cut, (i + 1) * cut, square, total, unroll=2)
    inv = lax.rsqrt(jnp.sum(total, axis=1, keepdims=True) / width + EPS)
    inv = jnp.broadcast_to(inv, (rows, lanes))
    started["gain"].wait()

    def normalize(z, carry):
        for ref, side in ((xo_ref, tp), (xp_ref, 1 - tp)):
            to = pl.ds(pl.multiple_of((2 * z + side) * lanes, lanes), lanes)
            normed_ref[:, to] = (block(ref, z, side) * inv * gain_ref[:, to]).astype(BF16)
        return carry

    lax.fori_loop(0, blocks, normalize, 0, unroll=2)
    for key in ("wk", "wv", "wq", "wo", "wi", "wf"):
        started[key].wait()
    normed = normed_ref[...]
    proj = dot_t(normed, at["w"][...])
    gates = dot_t(at["wg"][...], normed)
    for key in small:
        started[key].wait()
    bias_ref, hg_ref, acc_ref, pi_ref, pf_ref = (at[k] for k in ("bias", "hg", "acc", "pi", "pf"))
    stab_ref, pk_ref, pv_ref, nrm_ref = (at[k] for k in ("stab", "pk", "pv", "nrm"))
    nk_ref, nv_ref, ni_ref, nf_ref = (at[k] for k in ("nk", "nv", "ni", "nf"))
    msg_ref = hbm["msg"]

    new_k = proj[:, :keys].astype(BF16)
    new_v = proj[:, keys : keys + values].astype(BF16)
    nk_ref[...] = new_k
    nv_ref[...] = new_v
    send(nk_ref, hbm["nk"])
    send(nv_ref, hbm["nv"])
    query = proj[:, keys + values : 2 * keys + values].astype(BF16)
    out_gate = proj[:, 2 * keys + values :]
    scale = keys ** (-0.5)

    grow = iota(gates.shape, 0)
    gate_in = jnp.sum(jnp.where(grow == head, gates, 0.0), axis=0, keepdims=True)
    gate_forget = jnp.sum(jnp.where(grow == heads + head, gates, 0.0), axis=0, keepdims=True)
    shape = (2 * steps, rows)
    spread = jnp.where(iota(shape, 0) < steps, gate_in, gate_forget)
    spread = jnp.where(iota(shape, 1) % steps == iota(shape, 0) % steps, spread, 0.0)
    member = (iota((rows, seqs), 0) // steps == iota((rows, seqs), 1)).astype(F32).astype(BF16)
    compact = sum(dot(p, member) for p in split(spread, 3))
    bias = bias_ref[...]
    bias = jnp.sum(jnp.where(iota(bias.shape, 1) == head, bias, 0.0), axis=1, keepdims=True)
    new_in = compact[:steps]
    new_forget = log_sigmoid(compact[steps:] + bias)
    ni_ref[...] = new_in
    nf_ref[...] = new_forget
    send(ni_ref, hbm["ni"])
    send(nf_ref, hbm["nf"])
    old_in, old_forget = kept_gates(pi_ref[...], pf_ref[...], acc_ref[...])
    inflow = jnp.concatenate([old_in, new_in], axis=0)
    run = running_rows(jnp.concatenate([old_forget, new_forget], axis=0))
    running = jnp.concatenate(run, axis=0)
    stab = stab_ref[...]
    span = 2 * steps
    place = iota((span, seqs), 0)
    weights, carries, floors = [], [], []
    for t in range(steps):
        latest = run[steps + t]
        d = latest - running + inflow
        d = jnp.where(place <= steps + t, d, FAR_NEGATIVE)
        carried = latest + stab
        top = jnp.maximum(jnp.max(d, axis=0, keepdims=True), carried)
        weights.append(jnp.exp(d - top))
        carries.append(jnp.exp(carried - top))
        floors.append(jnp.exp(-top))

    stacked = jnp.concatenate(weights, axis=0)
    widened = sum(dot_t(p, member) for p in split(stacked, 3))
    keep = iota((span, rows), 0) % steps == iota((span, rows), 1) % steps
    rows_of = [
        jnp.where(keep, widened[t * span : (t + 1) * span], 0.0) for t in range(steps)
    ]
    old_coef = jnp.concatenate(
        [jnp.sum(r[:steps], axis=0, keepdims=True) for r in rows_of], axis=0
    )
    new_coef = jnp.concatenate(
        [jnp.sum(r[steps:], axis=0, keepdims=True) for r in rows_of], axis=0
    )

    def tiled(x, count):
        x = jnp.concatenate([x] * (8 // steps), axis=0)
        return jnp.concatenate([x] * (count // 8), axis=0)

    mine = iota((rows, seqs), 0) // steps == iota((rows, seqs), 1)
    carry_wide = jnp.where(mine, tiled(jnp.concatenate(carries, axis=0), rows), 0.0)
    floor_wide = jnp.where(mine, tiled(jnp.concatenate(floors, axis=0), rows), 0.0)
    carry_scale = jnp.sum(carry_wide, axis=1, keepdims=True)
    least = jnp.sum(floor_wide, axis=1, keepdims=True)
    normal = sum(dot_t(query, p) for p in split(nrm_ref[...], 3))
    carried_normal = jnp.sum(carry_wide * (normal * scale), axis=1, keepdims=True)

    half = rows // 2
    together = iota((half, half), 0) // steps == iota((half, half), 1) // steps
    old_k, old_v = pk_ref[...], pv_ref[...]
    numerators, denominators = [], []
    for h in range(2):
        part = slice(h * half, (h + 1) * half)
        q = query[part]
        numerator = jnp.zeros((half, values), F32)
        denominator = jnp.zeros((half, half), F32)
        for k, v, c in ((old_k, old_v, old_coef), (new_k, new_v, new_coef)):
            score = dot_t(q, k[part]) * scale
            w = jnp.where(together, tiled(c[:, part], half) * score, 0.0)
            denominator = denominator + w
            for p in split(w, 2):
                numerator = numerator + dot(p, v[part])
        numerators.append(numerator)
        denominators.append(jnp.sum(denominator, axis=1, keepdims=True))
    numerator = jnp.concatenate(numerators, axis=0)
    denominator = jnp.concatenate(denominators, axis=0) + carried_normal

    started["mem"].wait()
    group = 4
    span_rows = group * steps
    quarter = iota((span_rows, 2 * values), 0) // steps
    for g in range(seqs // group):
        block_of = mem_ref[g * group : (g + 1) * group].reshape(group * values, keys).astype(BF16)
        full = dot_t(query[g * span_rows : (g + 1) * span_rows, :], block_of)
        side = jnp.where(quarter < 2, full[:, : 2 * values], full[:, 2 * values :])
        mq_ref[g * span_rows : (g + 1) * span_rows, :] = jnp.where(
            quarter[:, :values] % 2 == 0, side[:, :values], side[:, values:]
        )
    numerator = numerator + carry_scale * (mq_ref[...] * scale)
    cell = numerator / jnp.maximum(jnp.abs(denominator), least)
    ones = jnp.ones((8, values), BF16)
    squares = sum(dot_t(ones, p) for p in split(cell * cell, 3))[0:1]
    full_gain = hg_ref[...]
    gain = jnp.sum(jnp.where(iota(full_gain.shape, 0) == head, full_gain, 0.0), axis=0, keepdims=True)
    gain = jnp.where(tp == 0, gain[:, :values], gain[:, values:])
    gated = jax.nn.sigmoid(out_gate) * cell * gain
    msg_ref[:half, :] = jnp.concatenate([gated[:half], gated[half:]], axis=1).astype(BF16)
    high = squares.astype(BF16).astype(F32)
    low = squares - high
    line = iota((PACK, half), 0)
    slab = jnp.where(line == 0, high[:, :half], 0.0)
    slab = jnp.where(line == 1, high[:, half:], slab)
    slab = jnp.where(line == 8, low[:, :half], slab)
    slab = jnp.where(line == 9, low[:, half:], slab)
    msg_ref[half:, :] = slab.astype(BF16)
    for copy in leaving:
        copy.wait()


def run_cell(*args):
    xo, rest, gain, wi = args[0], args[2], args[3], args[8]
    pi, pk, pv, nrm, mem = args[13], *args[16:20]
    rows, keys = pk.shape
    values = pv.shape[1]
    scratch = [pltpu.VMEM(a.shape, a.dtype) for a in (xo, xo, rest, gain)]
    scratch += [
        pltpu.VMEM((2 * keys + 2 * values, gain.shape[1]), BF16),
        pltpu.VMEM((2 * wi.shape[0], gain.shape[1]), BF16),
    ]
    scratch += [pltpu.VMEM(a.shape, a.dtype) for a in args[10:20]]
    scratch += [
        pltpu.VMEM((rows, gain.shape[1]), BF16),
        pltpu.VMEM((rows, values), F32),
        pltpu.VMEM((rows, keys), BF16),
        pltpu.VMEM((rows, values), BF16),
        pltpu.VMEM(pi.shape, F32),
        pltpu.VMEM(pi.shape, F32),
        pltpu.SemaphoreType.DMA((len(args) + 2 * CUTS + 4,)),
    ]
    return pl.pallas_call(
        cell_kernel,
        name="cell",
        out_shape=(
            jax.ShapeDtypeStruct((rows // 2 + PACK, 2 * values), BF16),
            jax.ShapeDtypeStruct((rows, keys), BF16),
            jax.ShapeDtypeStruct((rows, values), BF16),
            jax.ShapeDtypeStruct(pi.shape, F32),
            jax.ShapeDtypeStruct(pi.shape, F32),
        ),
        in_specs=[pl.BlockSpec(memory_space=pl.ANY)] * len(args),
        out_specs=(
            pl.BlockSpec(memory_space=pltpu.VMEM),
            *[pl.BlockSpec(memory_space=pl.ANY)] * 4,
        ),
        scratch_shapes=scratch,
        cost_estimate=pl.CostEstimate(flops=1500000000, bytes_accessed=8000000, transcendentals=100000),
        compiler_params=pltpu.CompilerParams(vmem_limit_bytes=53 * 1024 * 1024),
    )(*args)


def out_kernel(own_ref, other_ref, w_ref, out_ref):
    tp = lax.axis_index("tp")
    heads, tall, _ = own_ref.shape
    half = tall - PACK
    parts, _, chunk, feats = w_ref.shape
    values = parts * chunk
    slab = own_ref[:, half:, :].astype(F32) + other_ref[:, half:, :].astype(F32)
    squares = (slab[:, :8, :] + slab[:, 8:, :]).reshape(heads * 8, half)
    inv = lax.rsqrt(squares / (2 * values) + EPS).T
    zero = jnp.zeros((values, feats), BF16)
    low = jnp.zeros((half, feats), F32)
    high = jnp.zeros((half, feats), F32)
    for h in range(heads):
        sent = jnp.concatenate([own_ref[h, :half, :], other_ref[h, :half, :]], axis=1)
        mine = jnp.concatenate([w_ref[d, 2 * h + tp] for d in range(parts)], axis=0)
        theirs = jnp.concatenate([w_ref[d, 2 * h + 1 - tp] for d in range(parts)], axis=0)
        weight = jnp.concatenate(
            [
                jnp.concatenate([mine, zero, theirs, zero], axis=0),
                jnp.concatenate([zero, mine, zero, theirs], axis=0),
            ],
            axis=1,
        )
        both = dot(sent, weight)
        low = low + inv[:, 8 * h : 8 * h + 1] * both[:, :feats]
        high = high + inv[:, 8 * h + 1 : 8 * h + 2] * both[:, feats:]
    out_ref[:half, :] = low.astype(BF16)
    out_ref[half:, :] = high.astype(BF16)


def project_out(own, other, weight):
    rows = 2 * (own.shape[1] - PACK)
    return pl.pallas_call(
        out_kernel,
        name="mix",
        out_shape=jax.ShapeDtypeStruct((rows, weight.shape[3]), BF16),
        in_specs=[pl.BlockSpec(memory_space=pltpu.VMEM)] * 3,
        cost_estimate=pl.CostEstimate(flops=270000000, bytes_accessed=2000000, transcendentals=10000),
        compiler_params=pltpu.CompilerParams(vmem_limit_bytes=8 * 1024 * 1024),
    )(own, other, weight)


def swap(value, axis):
    size = lax.axis_size(axis)
    return lax.ppermute(value, axis, [(i, size - 1 - i) for i in range(size)])


def shards(
    tokens,
    norm_gain,
    w_query,
    w_key,
    w_value,
    w_outgate,
    w_input,
    w_forget,
    forget_bias,
    head_gain,
    w_out,
    memory,
    normalizer,
    stabilizer,
    prev_keys,
    prev_values,
    prev_input,
    prev_forget,
    accepted,
):
    seqs, steps, lanes = tokens.shape
    rows = seqs * steps
    keys, values = w_query.shape[2], w_value.shape[2]
    kv, tp, dp = lax.axis_size("kv"), lax.axis_size("tp"), lax.axis_size("dp")
    x = tokens.reshape(rows, lanes)
    main = rows - LAST
    share = min(dp, SHARE)
    chunk = values // share

    piece = lax.dynamic_slice_in_dim(w_out[0], lax.axis_index("dp") % share * chunk, chunk, 0)
    piece = piece.reshape(chunk, kv * tp, lanes).transpose(1, 0, 2)
    last = jnp.broadcast_to(x[main:][None], (kv * tp, LAST, lanes))
    packed = jnp.concatenate([last, piece], axis=1)
    first = lax.all_to_all(packed, ("kv", "tp"), 0, 0, tiled=True)
    own = lax.all_gather(x[:main], "kv")
    other = swap(own, "tp")
    piece = first[:, LAST:]
    piece = jnp.broadcast_to(piece[None], (share, *piece.shape))
    groups = [list(range(i, i + share)) for i in range(0, dp, share)]
    weight = lax.all_to_all(piece, "dp", 0, 0, tiled=True, axis_index_groups=groups)

    def turned(w):
        return w.transpose(1, 2, 0).reshape(-1, w.shape[0])

    acc = accepted.reshape(1, seqs)
    pi = prev_input.transpose(1, 2, 0).reshape(steps, seqs)
    pf = prev_forget.transpose(1, 2, 0).reshape(steps, seqs)
    stab = stabilizer.transpose(1, 0)
    pk = prev_keys.reshape(rows, keys)
    pv = prev_values.reshape(rows, values)
    nrm = normalizer.reshape(seqs, keys)
    mem = memory.reshape(seqs, values, keys)
    new_memory, new_normalizer, new_stabilizer = update_state(acc, pi, pf, stab, pk, pv, nrm, mem)
    msg, new_keys, new_values, new_input, new_forget = run_cell(
        own, other, first, norm_gain.reshape(1, -1),
        turned(w_key), turned(w_value), turned(w_query), turned(w_outgate), w_input.T, w_forget.T,
        forget_bias.reshape(1, -1), head_gain, acc, pi, pf, stab, pk, pv, nrm, mem,
    )
    gated = lax.all_gather(msg, "kv")
    mixed = project_out(gated, swap(gated, "tp"), weight)
    return (
        mixed.reshape(seqs, steps, lanes),
        new_memory.reshape(memory.shape),
        new_normalizer.reshape(normalizer.shape),
        new_stabilizer.transpose(1, 0),
        new_keys.reshape(prev_keys.shape),
        new_values.reshape(prev_values.shape),
        new_input.reshape(steps, 1, seqs).transpose(2, 0, 1),
        new_forget.reshape(steps, 1, seqs).transpose(2, 0, 1),
    )


def solution(mesh):
    specs = (
        P(("grp", "dp"), None, ("kv", "tp")),
        P(),
        P(None, "kv", None),
        P(None, "kv", None),
        P(None, "kv", "tp"),
        P(None, "kv", "tp"),
        P(),
        P(),
        P(),
        P(),
        P("kv", "tp", None),
        P(("grp", "dp"), "kv", "tp", None),
        P(("grp", "dp"), "kv", None),
        P(("grp", "dp"), "kv"),
        P(("grp", "dp"), None, "kv", None),
        P(("grp", "dp"), None, "kv", "tp"),
        P(("grp", "dp"), None, "kv"),
        P(("grp", "dp"), None, "kv"),
        P(("grp", "dp")),
    )
    outs = (
        P(("grp", "dp"), None, ("kv", "tp")),
        P(("grp", "dp"), "kv", "tp", None),
        P(("grp", "dp"), "kv", None),
        P(("grp", "dp"), "kv"),
        P(("grp", "dp"), None, "kv", None),
        P(("grp", "dp"), None, "kv", "tp"),
        P(("grp", "dp"), None, "kv"),
        P(("grp", "dp"), None, "kv"),
    )

    return jax.shard_map(shards, mesh=mesh, in_specs=specs, out_specs=outs, check_vma=False)
```

```python
import jax
import jax.numpy as jnp
from jax import lax
from jax.experimental import pallas as pl
from jax.experimental.pallas import tpu as pltpu
from jax.sharding import PartitionSpec as P


EPS = 1e-06
FAR_NEGATIVE = -1e30
F32 = jnp.float32
BF16 = jnp.bfloat16
STATE_CUTS = 2
CUTS = 4
SHARE = 8
LAST = 8
PACK = 16


def iota(shape, dim):
    return lax.broadcasted_iota(jnp.int32, shape, dim)


def dot(a, b, precision=None):
    return jnp.dot(a, b, preferred_element_type=F32, precision=precision)


def dot_t(a, b, precision=None):
    return lax.dot_general(
        a, b, (((1,), (1,)), ((), ())), preferred_element_type=F32, precision=precision
    )


def split(x, parts):
    pieces = []
    for _ in range(parts):
        piece = x.astype(BF16)
        pieces.append(piece)
        x = x - piece.astype(F32)
    return pieces


def log_sigmoid(x):
    return jnp.minimum(x, 0.0) - jnp.log1p(jnp.exp(-jnp.abs(x)))


def kept_gates(prev_in, prev_forget, accepted):
    dropped = iota(prev_in.shape, 0) >= accepted
    return jnp.where(dropped, FAR_NEGATIVE, prev_in), jnp.where(dropped, 0.0, prev_forget)


def running_rows(forget):
    rows = [forget[0:1]]
    for j in range(1, forget.shape[0]):
        rows.append(rows[-1] + forget[j : j + 1])
    return rows


def state_kernel(
    acc_ref, pi_ref, pf_ref, stab_ref, pk_ref, pv_ref, nrm_ref, mem_hbm,
    new_mem_hbm, new_nrm_ref, new_stab_ref, mem_ref, new_mem_ref, ks_ref, vt_ref, decay_ref,
    in_sem, out_sem,
):
    seqs, values, _ = mem_ref.shape
    steps = pi_ref.shape[0]
    rows = seqs * steps
    piece = seqs // STATE_CUTS
    parts = [pl.ds(i * piece, piece) for i in range(STATE_CUTS)]
    loads = [
        pltpu.make_async_copy(mem_hbm.at[p], mem_ref.at[p], in_sem.at[i])
        for i, p in enumerate(parts)
    ]
    stores = [
        pltpu.make_async_copy(new_mem_ref.at[p], new_mem_hbm.at[p], out_sem.at[i])
        for i, p in enumerate(parts)
    ]
    for copy in loads:
        copy.start()
    inflow, forget = kept_gates(pi_ref[...], pf_ref[...], acc_ref[...])
    running = running_rows(forget)
    edge = running[-1]
    stab = stab_ref[...]
    reached = [edge - running[j] + inflow[j : j + 1] for j in range(steps)]
    top = edge + stab
    for r in reached:
        top = jnp.maximum(top, r)
    new_stab_ref[...] = top
    decay = jnp.exp(edge + stab - top)
    row, lane = iota((rows, seqs), 0), iota((rows, seqs), 1)
    picked = jnp.zeros((rows, seqs), F32)
    for j in range(steps):
        picked = jnp.where(row == lane * steps + j, jnp.exp(reached[j] - top), picked)
    share_col = jnp.sum(picked, axis=1, keepdims=True)
    same = iota((seqs, seqs), 0) == iota((seqs, seqs), 1)
    decay_col = jnp.sum(jnp.where(same, decay, 0.0), axis=1, keepdims=True)
    decay_ref[...] = jnp.broadcast_to(decay_col, decay_ref.shape)
    scaled = pk_ref[...].astype(F32) * share_col
    ks_ref[...] = scaled.astype(BF16)
    vt_ref[...] = pv_ref[...].astype(F32).T.astype(BF16)
    member = (iota((seqs, rows), 1) // steps == iota((seqs, rows), 0)).astype(F32).astype(BF16)
    new_nrm_ref[...] = decay_col * nrm_ref[...] + sum(dot(member, p) for p in split(scaled, 3))
    wide = 128 // steps
    group = 4
    owner = iota((values, 128), 1) // steps
    for i in range(STATE_CUTS):
        half = i * piece // wide
        first = i * piece % wide
        ks = ks_ref[half * 128 : (half + 1) * 128, :]
        vt = vt_ref[:, half * 128 : (half + 1) * 128]
        loads[i].wait()
        for g in range(piece // group):
            masks = [
                jnp.where(owner == first + g * group + n, vt, jnp.zeros_like(vt))
                for n in range(group)
            ]
            added = dot(jnp.concatenate(masks, axis=0), ks)
            for n in range(group):
                s = i * piece + g * group + n
                new_mem_ref[s] = (
                    decay_ref[s : s + 1, :] * mem_ref[s]
                    + added[n * values : (n + 1) * values, :]
                )
        stores[i].start()
    for copy in stores:
        copy.wait()


def update_state(accepted, prev_in, prev_forget, stab, pk, pv, normalizer, memory):
    seqs, values, keys = memory.shape
    rows = pk.shape[0]
    vmem = pl.BlockSpec(memory_space=pltpu.VMEM)
    return pl.pallas_call(
        state_kernel,
        name="state",
        out_shape=(
            jax.ShapeDtypeStruct(memory.shape, F32),
            jax.ShapeDtypeStruct(normalizer.shape, F32),
            jax.ShapeDtypeStruct(stab.shape, F32),
        ),
        in_specs=[vmem] * 7 + [pl.BlockSpec(memory_space=pl.ANY)],
        out_specs=(pl.BlockSpec(memory_space=pl.ANY), vmem, vmem),
        scratch_shapes=[
            pltpu.VMEM(memory.shape, F32),
            pltpu.VMEM(memory.shape, F32),
            pltpu.VMEM((rows, keys), BF16),
            pltpu.VMEM((values, rows), BF16),
            pltpu.VMEM((seqs, keys), F32),
            pltpu.SemaphoreType.DMA((STATE_CUTS,)),
            pltpu.SemaphoreType.DMA((STATE_CUTS,)),
        ],
        cost_estimate=pl.CostEstimate(flops=200000000, bytes_accessed=4500000, transcendentals=400),
        compiler_params=pltpu.CompilerParams(vmem_limit_bytes=12 * 1024 * 1024),
    )(accepted, prev_in, prev_forget, stab, pk, pv, normalizer, memory)


def cell_kernel(*refs):
    names = ("xo", "xp", "rest", "gain", "wk", "wv", "wq", "wo", "wi", "wf", "bias", "hg", "acc")
    names += ("pi", "pf", "stab", "pk", "pv", "nrm", "mem", "msg", "nk", "nv", "ni", "nf")
    hbm = dict(zip(names, refs))
    near = list(refs[len(names) :])
    sems = near.pop()
    leaving = []

    def send(src, dst):
        leaving.append(pltpu.make_async_copy(src, dst, sems.at[len(started) + len(leaving)]))
        leaving[-1].start()

    order = ("xo", "xp", "rest", "gain", "w", "wg", "bias", "hg", "acc", "pi", "pf", "stab")
    order += ("pk", "pv", "nrm", "mem", "normed", "mq", "nk", "nv", "ni", "nf")
    at = dict(zip(order, near))
    tp, head = lax.axis_index("tp"), lax.axis_index("kv")
    xo_ref, xp_ref, rest_ref, gain_ref = at["xo"], at["xp"], at["rest"], at["gain"]
    normed_ref, mem_ref, mq_ref = at["normed"], at["mem"], at["mq"]
    blocks, main, lanes = xo_ref.shape
    seqs, values, keys = mem_ref.shape
    steps = at["pi"].shape[0]
    rows = seqs * steps
    heads = at["wg"].shape[0] // 2
    width = gain_ref.shape[1]
    cut = blocks // CUTS
    started = {}

    def bring(key, src, dst):
        started[key] = pltpu.make_async_copy(src, dst, sems.at[len(started)])
        started[key].start()

    bring("rest", hbm["rest"], rest_ref)
    for i in range(CUTS):
        part = pl.ds(i * cut, cut)
        bring(("xo", i), hbm["xo"].at[part], xo_ref.at[part])
        bring(("xp", i), hbm["xp"].at[part], xp_ref.at[part])
    bring("gain", hbm["gain"], gain_ref)
    for i, key in enumerate(("wk", "wv", "wq", "wo")):
        bring(key, hbm[key], at["w"].at[pl.ds(i * keys, keys)])
    for i, key in enumerate(("wi", "wf")):
        bring(key, hbm[key], at["wg"].at[pl.ds(i * heads, heads)])
    small = ("bias", "hg", "acc", "pi", "pf", "stab", "pk", "pv", "nrm")
    for key in (*small, "mem"):
        bring(key, hbm[key], at[key])

    def block(ref, z, side):
        low = rest_ref[2 * z + side]
        return jnp.concatenate([ref[z].astype(F32), low.astype(F32)[: rows - main]], axis=0)

    def square(z, total):
        a, b = block(xo_ref, z, tp), block(xp_ref, z, 1 - tp)
        return total + (a * a + b * b)

    total = jnp.zeros((rows, lanes), F32)
    started["rest"].wait()
    for i in range(CUTS):
        started["xo", i].wait()
        started["xp", i].wait()
        total = lax.fori_loop(i * cut, (i + 1) * cut, square, total, unroll=2)
    inv = lax.rsqrt(jnp.sum(total, axis=1, keepdims=True) / width + EPS)
    inv = jnp.broadcast_to(inv, (rows, lanes))
    started["gain"].wait()

    def normalize(z, carry):
        for ref, side in ((xo_ref, tp), (xp_ref, 1 - tp)):
            to = pl.ds(pl.multiple_of((2 * z + side) * lanes, lanes), lanes)
            normed_ref[:, to] = (block(ref, z, side) * inv * gain_ref[:, to]).astype(BF16)
        return carry

    lax.fori_loop(0, blocks, normalize, 0, unroll=2)
    for key in ("wk", "wv", "wq", "wo", "wi", "wf"):
        started[key].wait()
    normed = normed_ref[...]
    proj = dot_t(normed, at["w"][...])
    gates = dot_t(at["wg"][...], normed)
    for key in small:
        started[key].wait()
    bias_ref, hg_ref, acc_ref, pi_ref, pf_ref = (at[k] for k in ("bias", "hg", "acc", "pi", "pf"))
    stab_ref, pk_ref, pv_ref, nrm_ref = (at[k] for k in ("stab", "pk", "pv", "nrm"))
    nk_ref, nv_ref, ni_ref, nf_ref = (at[k] for k in ("nk", "nv", "ni", "nf"))
    msg_ref = hbm["msg"]

    new_k = proj[:, :keys].astype(BF16)
    new_v = proj[:, keys : keys + values].astype(BF16)
    nk_ref[...] = new_k
    nv_ref[...] = new_v
    send(nk_ref, hbm["nk"])
    send(nv_ref, hbm["nv"])
    query = proj[:, keys + values : 2 * keys + values].astype(BF16)
    out_gate = proj[:, 2 * keys + values :]
    scale = keys ** (-0.5)

    grow = iota(gates.shape, 0)
    gate_in = jnp.sum(jnp.where(grow == head, gates, 0.0), axis=0, keepdims=True)
    gate_forget = jnp.sum(jnp.where(grow == heads + head, gates, 0.0), axis=0, keepdims=True)
    shape = (2 * steps, rows)
    spread = jnp.where(iota(shape, 0) < steps, gate_in, gate_forget)
    spread = jnp.where(iota(shape, 1) % steps == iota(shape, 0) % steps, spread, 0.0)
    member = (iota((rows, seqs), 0) // steps == iota((rows, seqs), 1)).astype(F32).astype(BF16)
    compact = sum(dot(p, member) for p in split(spread, 3))
    bias = bias_ref[...]
    bias = jnp.sum(jnp.where(iota(bias.shape, 1) == head, bias, 0.0), axis=1, keepdims=True)
    new_in = compact[:steps]
    new_forget = log_sigmoid(compact[steps:] + bias)
    ni_ref[...] = new_in
    nf_ref[...] = new_forget
    send(ni_ref, hbm["ni"])
    send(nf_ref, hbm["nf"])
    old_in, old_forget = kept_gates(pi_ref[...], pf_ref[...], acc_ref[...])
    inflow = jnp.concatenate([old_in, new_in], axis=0)
    run = running_rows(jnp.concatenate([old_forget, new_forget], axis=0))
    running = jnp.concatenate(run, axis=0)
    stab = stab_ref[...]
    span = 2 * steps
    place = iota((span, seqs), 0)
    weights, carries, floors = [], [], []
    for t in range(steps):
        latest = run[steps + t]
        d = latest - running + inflow
        d = jnp.where(place <= steps + t, d, FAR_NEGATIVE)
        carried = latest + stab
        top = jnp.maximum(jnp.max(d, axis=0, keepdims=True), carried)
        weights.append(jnp.exp(d - top))
        carries.append(jnp.exp(carried - top))
        floors.append(jnp.exp(-top))

    stacked = jnp.concatenate(weights, axis=0)
    widened = sum(dot_t(p, member) for p in split(stacked, 3))
    keep = iota((span, rows), 0) % steps == iota((span, rows), 1) % steps
    rows_of = [
        jnp.where(keep, widened[t * span : (t + 1) * span], 0.0) for t in range(steps)
    ]
    old_coef = jnp.concatenate(
        [jnp.sum(r[:steps], axis=0, keepdims=True) for r in rows_of], axis=0
    )
    new_coef = jnp.concatenate(
        [jnp.sum(r[steps:], axis=0, keepdims=True) for r in rows_of], axis=0
    )

    def tiled(x, count):
        x = jnp.concatenate([x] * (8 // steps), axis=0)
        return jnp.concatenate([x] * (count // 8), axis=0)

    mine = iota((rows, seqs), 0) // steps == iota((rows, seqs), 1)
    carry_wide = jnp.where(mine, tiled(jnp.concatenate(carries, axis=0), rows), 0.0)
    floor_wide = jnp.where(mine, tiled(jnp.concatenate(floors, axis=0), rows), 0.0)
    carry_scale = jnp.sum(carry_wide, axis=1, keepdims=True)
    least = jnp.sum(floor_wide, axis=1, keepdims=True)
    normal = sum(dot_t(query, p) for p in split(nrm_ref[...], 3))
    carried_normal = jnp.sum(carry_wide * (normal * scale), axis=1, keepdims=True)

    half = rows // 2
    together = iota((half, half), 0) // steps == iota((half, half), 1) // steps
    old_k, old_v = pk_ref[...], pv_ref[...]
    numerators, denominators = [], []
    for h in range(2):
        part = slice(h * half, (h + 1) * half)
        q = query[part]
        numerator = jnp.zeros((half, values), F32)
        denominator = jnp.zeros((half, half), F32)
        for k, v, c in ((old_k, old_v, old_coef), (new_k, new_v, new_coef)):
            score = dot_t(q, k[part]) * scale
            w = jnp.where(together, tiled(c[:, part], half) * score, 0.0)
            denominator = denominator + w
            for p in split(w, 2):
                numerator = numerator + dot(p, v[part])
        numerators.append(numerator)
        denominators.append(jnp.sum(denominator, axis=1, keepdims=True))
    numerator = jnp.concatenate(numerators, axis=0)
    denominator = jnp.concatenate(denominators, axis=0) + carried_normal

    started["mem"].wait()
    group = 4
    span_rows = group * steps
    quarter = iota((span_rows, 2 * values), 0) // steps
    for g in range(seqs // group):
        block_of = mem_ref[g * group : (g + 1) * group].reshape(group * values, keys).astype(BF16)
        full = dot_t(query[g * span_rows : (g + 1) * span_rows, :], block_of)
        side = jnp.where(quarter < 2, full[:, : 2 * values], full[:, 2 * values :])
        mq_ref[g * span_rows : (g + 1) * span_rows, :] = jnp.where(
            quarter[:, :values] % 2 == 0, side[:, :values], side[:, values:]
        )
    numerator = numerator + carry_scale * (mq_ref[...] * scale)
    cell = numerator / jnp.maximum(jnp.abs(denominator), least)
    ones = jnp.ones((8, values), BF16)
    squares = sum(dot_t(ones, p) for p in split(cell * cell, 3))[0:1]
    full_gain = hg_ref[...]
    gain = jnp.sum(jnp.where(iota(full_gain.shape, 0) == head, full_gain, 0.0), axis=0, keepdims=True)
    gain = jnp.where(tp == 0, gain[:, :values], gain[:, values:])
    gated = jax.nn.sigmoid(out_gate) * cell * gain
    msg_ref[:half, :] = jnp.concatenate([gated[:half], gated[half:]], axis=1).astype(BF16)
    high = squares.astype(BF16).astype(F32)
    low = squares - high
    line = iota((PACK, half), 0)
    slab = jnp.where(line == 0, high[:, :half], 0.0)
    slab = jnp.where(line == 1, high[:, half:], slab)
    slab = jnp.where(line == 8, low[:, :half], slab)
    slab = jnp.where(line == 9, low[:, half:], slab)
    msg_ref[half:, :] = slab.astype(BF16)
    for copy in leaving:
        copy.wait()


def run_cell(*args):
    xo, rest, gain, wi = args[0], args[2], args[3], args[8]
    pi, pk, pv, nrm, mem = args[13], *args[16:20]
    rows, keys = pk.shape
    values = pv.shape[1]
    scratch = [pltpu.VMEM(a.shape, a.dtype) for a in (xo, xo, rest, gain)]
    scratch += [
        pltpu.VMEM((2 * keys + 2 * values, gain.shape[1]), BF16),
        pltpu.VMEM((2 * wi.shape[0], gain.shape[1]), BF16),
    ]
    scratch += [pltpu.VMEM(a.shape, a.dtype) for a in args[10:20]]
    scratch += [
        pltpu.VMEM((rows, gain.shape[1]), BF16),
        pltpu.VMEM((rows, values), F32),
        pltpu.VMEM((rows, keys), BF16),
        pltpu.VMEM((rows, values), BF16),
        pltpu.VMEM(pi.shape, F32),
        pltpu.VMEM(pi.shape, F32),
        pltpu.SemaphoreType.DMA((len(args) + 2 * CUTS + 4,)),
    ]
    return pl.pallas_call(
        cell_kernel,
        name="cell",
        out_shape=(
            jax.ShapeDtypeStruct((rows // 2 + PACK, 2 * values), BF16),
            jax.ShapeDtypeStruct((rows, keys), BF16),
            jax.ShapeDtypeStruct((rows, values), BF16),
            jax.ShapeDtypeStruct(pi.shape, F32),
            jax.ShapeDtypeStruct(pi.shape, F32),
        ),
        in_specs=[pl.BlockSpec(memory_space=pl.ANY)] * len(args),
        out_specs=(
            pl.BlockSpec(memory_space=pltpu.VMEM),
            *[pl.BlockSpec(memory_space=pl.ANY)] * 4,
        ),
        scratch_shapes=scratch,
        cost_estimate=pl.CostEstimate(flops=1500000000, bytes_accessed=8000000, transcendentals=100000),
        compiler_params=pltpu.CompilerParams(vmem_limit_bytes=53 * 1024 * 1024),
    )(*args)


def out_kernel(own_ref, other_ref, w_ref, out_ref):
    tp = lax.axis_index("tp")
    heads, tall, _ = own_ref.shape
    half = tall - PACK
    parts, _, chunk, feats = w_ref.shape
    values = parts * chunk
    slab = own_ref[:, half:, :].astype(F32) + other_ref[:, half:, :].astype(F32)
    squares = (slab[:, :8, :] + slab[:, 8:, :]).reshape(heads * 8, half)
    inv = lax.rsqrt(squares / (2 * values) + EPS).T
    zero = jnp.zeros((values, feats), BF16)
    low = jnp.zeros((half, feats), F32)
    high = jnp.zeros((half, feats), F32)
    for h in range(heads):
        sent = jnp.concatenate([own_ref[h, :half, :], other_ref[h, :half, :]], axis=1)
        mine = jnp.concatenate([w_ref[d, 2 * h + tp] for d in range(parts)], axis=0)
        theirs = jnp.concatenate([w_ref[d, 2 * h + 1 - tp] for d in range(parts)], axis=0)
        weight = jnp.concatenate(
            [
                jnp.concatenate([mine, zero, theirs, zero], axis=0),
                jnp.concatenate([zero, mine, zero, theirs], axis=0),
            ],
            axis=1,
        )
        both = dot(sent, weight)
        low = low + inv[:, 8 * h : 8 * h + 1] * both[:, :feats]
        high = high + inv[:, 8 * h + 1 : 8 * h + 2] * both[:, feats:]
    out_ref[:half, :] = low.astype(BF16)
    out_ref[half:, :] = high.astype(BF16)


def project_out(own, other, weight):
    rows = 2 * (own.shape[1] - PACK)
    return pl.pallas_call(
        out_kernel,
        name="mix",
        out_shape=jax.ShapeDtypeStruct((rows, weight.shape[3]), BF16),
        in_specs=[pl.BlockSpec(memory_space=pltpu.VMEM)] * 3,
        cost_estimate=pl.CostEstimate(flops=270000000, bytes_accessed=2000000, transcendentals=10000),
        compiler_params=pltpu.CompilerParams(vmem_limit_bytes=8 * 1024 * 1024),
    )(own, other, weight)


def swap(value, axis):
    size = lax.axis_size(axis)
    return lax.ppermute(value, axis, [(i, size - 1 - i) for i in range(size)])


def shards(
    tokens,
    norm_gain,
    w_query,
    w_key,
    w_value,
    w_outgate,
    w_input,
    w_forget,
    forget_bias,
    head_gain,
    w_out,
    memory,
    normalizer,
    stabilizer,
    prev_keys,
    prev_values,
    prev_input,
    prev_forget,
    accepted,
):
    seqs, steps, lanes = tokens.shape
    rows = seqs * steps
    keys, values = w_query.shape[2], w_value.shape[2]
    kv, tp, dp = lax.axis_size("kv"), lax.axis_size("tp"), lax.axis_size("dp")
    x = tokens.reshape(rows, lanes)
    main = rows - LAST
    share = min(dp, SHARE)
    chunk = values // share

    tail, behind = lax.optimization_barrier((x[main:], w_out[0]))
    piece = lax.dynamic_slice_in_dim(behind, lax.axis_index("dp") % share * chunk, chunk, 0)
    piece = piece.reshape(chunk, kv * tp, lanes).transpose(1, 0, 2)
    last = jnp.broadcast_to(tail[None], (kv * tp, LAST, lanes))
    packed = jnp.concatenate([last, piece], axis=1)
    first = lax.all_to_all(packed, ("kv", "tp"), 0, 0, tiled=True)
    own = lax.all_gather(x[:main], "kv")
    other = swap(own, "tp")
    piece = first[:, LAST:]
    piece = jnp.broadcast_to(piece[None], (share, *piece.shape))
    groups = [list(range(i, i + share)) for i in range(0, dp, share)]
    weight = lax.all_to_all(piece, "dp", 0, 0, tiled=True, axis_index_groups=groups)

    def turned(w):
        return w.transpose(1, 2, 0).reshape(-1, w.shape[0])

    acc = accepted.reshape(1, seqs)
    pi = prev_input.transpose(1, 2, 0).reshape(steps, seqs)
    pf = prev_forget.transpose(1, 2, 0).reshape(steps, seqs)
    stab = stabilizer.transpose(1, 0)
    pk = prev_keys.reshape(rows, keys)
    pv = prev_values.reshape(rows, values)
    nrm = normalizer.reshape(seqs, keys)
    mem = memory.reshape(seqs, values, keys)
    new_memory, new_normalizer, new_stabilizer = update_state(acc, pi, pf, stab, pk, pv, nrm, mem)
    msg, new_keys, new_values, new_input, new_forget = run_cell(
        own, other, first, norm_gain.reshape(1, -1),
        turned(w_key), turned(w_value), turned(w_query), turned(w_outgate), w_input.T, w_forget.T,
        forget_bias.reshape(1, -1), head_gain, acc, pi, pf, stab, pk, pv, nrm, mem,
    )
    gated = lax.all_gather(msg, "kv")
    mixed = project_out(gated, swap(gated, "tp"), weight)
    return (
        mixed.reshape(seqs, steps, lanes),
        new_memory.reshape(memory.shape),
        new_normalizer.reshape(normalizer.shape),
        new_stabilizer.transpose(1, 0),
        new_keys.reshape(prev_keys.shape),
        new_values.reshape(prev_values.shape),
        new_input.reshape(steps, 1, seqs).transpose(2, 0, 1),
        new_forget.reshape(steps, 1, seqs).transpose(2, 0, 1),
    )


def solution(mesh):
    specs = (
        P(("grp", "dp"), None, ("kv", "tp")),
        P(),
        P(None, "kv", None),
        P(None, "kv", None),
        P(None, "kv", "tp"),
        P(None, "kv", "tp"),
        P(),
        P(),
        P(),
        P(),
        P("kv", "tp", None),
        P(("grp", "dp"), "kv", "tp", None),
        P(("grp", "dp"), "kv", None),
        P(("grp", "dp"), "kv"),
        P(("grp", "dp"), None, "kv", None),
        P(("grp", "dp"), None, "kv", "tp"),
        P(("grp", "dp"), None, "kv"),
        P(("grp", "dp"), None, "kv"),
        P(("grp", "dp")),
    )
    outs = (
        P(("grp", "dp"), None, ("kv", "tp")),
        P(("grp", "dp"), "kv", "tp", None),
        P(("grp", "dp"), "kv", None),
        P(("grp", "dp"), "kv"),
        P(("grp", "dp"), None, "kv", None),
        P(("grp", "dp"), None, "kv", "tp"),
        P(("grp", "dp"), None, "kv"),
        P(("grp", "dp"), None, "kv"),
    )

    return jax.shard_map(shards, mesh=mesh, in_specs=specs, out_specs=outs, check_vma=False)
```
